256 devices in a mesh: sp: 64 (over z, y, core), tp: 4 (over x).
Axes of the slice: x: 4, y: 4, z: 8, core: 2. Of those that a mesh axis runs over, the one named last changes fastest.
Arguments:
- queries_one: bfloat16 [16384, 512], P('sp', 'tp'), may hold values from -6 to 6
- queries_two: bfloat16 [16384, 512], P('sp', 'tp'), may hold values from -6 to 6
- keys_one: bfloat16 [16384, 512], P('sp', 'tp'), may hold values from -6 to 6
- keys_two: bfloat16 [16384, 512], P('sp', 'tp'), may hold values from -6 to 6
- values: bfloat16 [16384, 1024], P('sp', 'tp'), may hold values from -6 to 6
- mix_lambda: float32 [4], P('tp'), may hold values from 0.3 to 0.8
- head_gain: float32 [1024], P('tp'), may hold values from 0.1 to 1.9
- out_weight: bfloat16 [1024, 2048], P('tp'), may hold values from -0.1875 to 0.1875
- residual_in: bfloat16 [16384, 2048], P('sp', 'tp'), may hold values from -12 to 12
- norm_gain: float32 [2048], replicated, may hold values from 0.1 to 1.9
- gate_weight: bfloat16 [2048, 5632], P('sp', 'tp'), may hold values from -0.125 to 0.125
- up_weight: bfloat16 [2048, 5632], P('sp', 'tp'), may hold values from -0.125 to 0.125
- down_weight: bfloat16 [5632, 2048], P('tp', 'sp'), may hold values from -0.078125 to 0.078125
Outputs:
- layer_out: bfloat16 [16384, 2048], P('sp', 'tp')
The draws below stay inside these ranges and needn't reach their ends.
All inputs are finite; a program needn't handle non-finite values.
Results may differ from the reference program's by a relative error of at most 0.012.
Values may be sent and summed in bfloat16 or wider, within the bound.
No kernel may reach another device: no remote copies, remote signals or barrier semaphores. Data moves between devices by JAX's collectives and lax.ppermute only.
A program may use at most 192 MiB of HBM per device.

```python
import math
import jax
import jax.numpy as jnp
from jax import lax

D = 2048
HEADS = 4
HEAD = 128
VALUE = 256
FF = 5632
SEQ = 16384
N_TP = 4


def planted(key, salt, pattern_salt, query_side):
    columns = HEADS * HEAD
    noise = 1.3 * jax.random.normal(jax.random.fold_in(key, salt), (SEQ, columns), jnp.float32)
    noise = jnp.clip(noise, -6.0, 6.0)
    return noise.astype(jnp.bfloat16)


def draw_queries_one(key, part):
    return planted(key, 1, 71, True)


def draw_keys_one(key, part):
    return planted(key, 2, 71, False)


def draw_queries_two(key, part):
    return planted(key, 3, 72, True)


def draw_keys_two(key, part):
    return planted(key, 4, 72, False)


def draw_residual_in(key, part):
    order = jax.random.permutation(jax.random.fold_in(key, 11), 4)
    column = jnp.arange(D, dtype=jnp.int32)
    quarter = column * 4 // D
    level = order[quarter].astype(jnp.float32)
    scales = 0.4 + 0.55 * level
    noise = jax.random.normal(jax.random.fold_in(key, 12), (SEQ, D), jnp.float32) * scales[None, :]
    return jnp.clip(noise, -12.0, 12.0).astype(jnp.bfloat16)


def shard_levels(own_key, shape, cuts, least, top_value):
    def one(position, blocks):
        steps = jax.random.uniform(jax.random.fold_in(jax.random.fold_in(own_key, 6), position), (blocks,), jnp.float32, least / len(cuts), top_value / len(cuts))
        return jnp.repeat(jnp.exp(steps), shape[position] // blocks).reshape((-1,) + (1,) * (len(shape) - position - 1))

    gain = one(*cuts[0])
    for cut in cuts[1:]:
        gain = gain * one(*cut)
    return gain


def scatter_about(key, extent, scale, bound, cuts=(), kind=jnp.bfloat16):
    drawn = jax.random.normal(key, extent, jnp.float32) * scale
    if len(cuts) > 0:
        drawn = shard_levels(key, extent, cuts, -0.22, 0.18) * drawn
    return jnp.clip(drawn, min=-bound, max=bound).astype(kind)


def setup_inputs(seed: int = 0) -> dict:
    keys = jax.random.split(jax.random.key(seed), 14)
    return {
        "queries_one": draw_queries_one(jax.random.fold_in(keys[13], 71), 0),
        "queries_two": draw_queries_two(jax.random.fold_in(keys[13], 71), 0),
        "keys_one": draw_keys_one(jax.random.fold_in(keys[13], 71), 0),
        "keys_two": draw_keys_two(jax.random.fold_in(keys[13], 71), 0),
        "values": scatter_about(keys[4], (SEQ, HEADS * VALUE), 1.0, 6.0, ((0, 64), (1, 4))),
        "mix_lambda": jnp.clip(0.3 + 0.5 * jax.random.uniform(keys[5], (HEADS,), jnp.float32) ** shard_levels(keys[5], (HEADS,), ((0, 4),), -0.2, 0.2), 0.3, 0.8),
        "head_gain": jnp.clip(1.0 + 0.18 * jax.random.normal(keys[6], (HEADS * VALUE,), jnp.float32), 0.1, 1.9),
        "out_weight": scatter_about(keys[7], (HEADS * VALUE, D), (HEADS * VALUE) ** -0.5, 0.1875, ((0, 4),)),
        "residual_in": draw_residual_in(jax.random.fold_in(keys[13], 71), 0),
        "norm_gain": jnp.clip(1.0 + 0.18 * jax.random.normal(keys[9], (D,), jnp.float32), 0.1, 1.9),
        "gate_weight": scatter_about(keys[10], (D, FF), D ** -0.5, 0.125, ((0, 64), (1, 4))),
        "up_weight": scatter_about(keys[11], (D, FF), D ** -0.5, 0.125, ((0, 64), (1, 4))),
        "down_weight": scatter_about(keys[12], (FF, D), FF ** -0.5, 0.078125, ((0, 4), (1, 64))),
    }


epsilon = 1e-06

def head_maps(query_one, query_two, key_one, key_two, value_rows, lam_head):
    seq_len = query_one.shape[0]
    block_rows = math.gcd(seq_len, 512)
    score_scale = HEAD ** (-0.5)
    key_pos = jnp.arange(seq_len, dtype=jnp.int32)

    def one_block(block_index):
        first_row = (block_index * block_rows).astype(jnp.int32)
        query_pos = first_row + jnp.arange(block_rows, dtype=jnp.int32)
        visible = key_pos[None, :] <= query_pos[:, None]

        def one_map(queries, key_rows):
            picked = lax.dynamic_slice_in_dim(queries, first_row, block_rows, 0)
            scores = jnp.dot(picked, key_rows.T, preferred_element_type=jnp.float32) * score_scale
            scores = jnp.where(visible, scores, -jnp.inf)
            highest = lax.optimization_barrier(jnp.max(scores, axis=1, keepdims=True))
            weights_exp = jnp.exp(scores - highest)
            totals = lax.optimization_barrier(jnp.sum(weights_exp, axis=1, keepdims=True))
            return jnp.dot(weights_exp.astype(jnp.bfloat16), value_rows, preferred_element_type=jnp.float32) / totals
        return one_map(query_one, key_one) - lam_head * one_map(query_two, key_two)
    blocks = lax.map(one_block, jnp.arange(seq_len // block_rows, dtype=jnp.int32))
    return blocks.reshape(seq_len, VALUE)

def rounded_sum(left, right, groups):
    width = left.shape[1] // groups
    result = jnp.zeros((left.shape[0], right.shape[1]), jnp.float32)
    for group in range(groups):
        partial_bf = jnp.dot(left[:, group * width:(group + 1) * width], right[group * width:(group + 1) * width], preferred_element_type=jnp.float32).astype(jnp.bfloat16)
        partial_bf = lax.optimization_barrier(partial_bf)
        result = result + partial_bf.astype(jnp.float32)
    return result

def reference(queries_one, queries_two, keys_one, keys_two, values, mix_lambda, head_gain, out_weight, residual_in, norm_gain, gate_weight, up_weight, down_weight):
    pieces = []
    for head_index in range(HEADS):
        qcols = slice(head_index * HEAD, (head_index + 1) * HEAD)
        vcols = slice(head_index * VALUE, (head_index + 1) * VALUE)
        mixed = head_maps(queries_one[:, qcols], queries_two[:, qcols], keys_one[:, qcols], keys_two[:, qcols], values[:, vcols], mix_lambda[head_index])
        mean_square = lax.optimization_barrier(jnp.mean(mixed * mixed, axis=1, keepdims=True))
        normed_head = mixed * lax.rsqrt(mean_square + epsilon) * head_gain[vcols][None, :] * 0.8
        pieces.append(normed_head.astype(jnp.bfloat16))
    attended = jnp.concatenate(pieces, axis=1)
    projected = rounded_sum(attended, out_weight, N_TP)
    resid = (residual_in.astype(jnp.float32) + projected).astype(jnp.bfloat16)
    resid_float = resid.astype(jnp.float32)
    mean_square = lax.optimization_barrier(jnp.mean(resid_float * resid_float, axis=1, keepdims=True))
    normed = (resid_float * lax.rsqrt(mean_square + epsilon) * norm_gain[None, :]).astype(jnp.bfloat16)
    gate_act = jnp.dot(normed, gate_weight, preferred_element_type=jnp.float32)
    up_act = jnp.dot(normed, up_weight, preferred_element_type=jnp.float32)
    hidden = (jax.nn.silu(gate_act) * up_act).astype(jnp.bfloat16)
    mlp_out = rounded_sum(hidden, down_weight, N_TP)
    return (resid_float + mlp_out).astype(jnp.bfloat16)
```

```python
import functools
import math

import jax
import jax.numpy as jnp
from jax import lax
from jax.experimental import pallas as pl
from jax.experimental.pallas import tpu as pltpu
from jax.sharding import Mesh
from jax.sharding import PartitionSpec as P

HEAD = 128
EPS = 1e-06
NEG = -1e30
FLOOR = -1e20
SCALE2 = HEAD**-0.5 * math.log2(math.e)
STAT = 16


VMEM = pl.BlockSpec(memory_space=pltpu.VMEM)
SMEM = pl.BlockSpec(memory_space=pltpu.SMEM)


def shift(a, axis, count, by):
    return lax.ppermute(a, axis, [(i, (i + by) % count) for i in range(count)])


def dot_nt(a, b):
    return lax.dot_general(a, b, (((1,), (1,)), ((), ())), preferred_element_type=jnp.float32)


def dot_nn(a, b):
    return lax.dot_general(a, b, (((1,), (0,)), ((), ())), preferred_element_type=jnp.float32)


def eye(n):
    return lax.broadcasted_iota(jnp.int32, (n, n), 0) == lax.broadcasted_iota(jnp.int32, (n, n), 1)


def to_row(col):
    n = col.shape[0]
    return jnp.sum(jnp.where(eye(n), col, 0.0), axis=0, keepdims=True)


def to_col(row):
    n = row.shape[1]
    return jnp.sum(jnp.where(eye(n), row, 0.0), axis=1, keepdims=True)


def stat_rows(lse_cols):
    row = jnp.concatenate([to_row(c) for c in lse_cols], axis=1)
    high = row.astype(jnp.bfloat16)
    rest = row - high.astype(jnp.float32)
    mid = rest.astype(jnp.bfloat16)
    low = (rest - mid.astype(jnp.float32)).astype(jnp.bfloat16)
    index = lax.broadcasted_iota(jnp.int32, (STAT, row.shape[1]), 0)
    zero = jnp.zeros_like(row)
    picked = jnp.where(
        index == 0,
        high.astype(jnp.float32),
        jnp.where(index == 1, mid.astype(jnp.float32), jnp.where(index == 2, low.astype(jnp.float32), zero)),
    )
    return picked.astype(jnp.bfloat16)


def read_stats(block):
    rows = block.shape[0] - STAT
    stats = block[rows:, :].astype(jnp.float32)
    row = jnp.sum(stats, axis=0, keepdims=True)
    half = row.shape[1] // 2
    return to_col(row[:, :half]), to_col(row[:, half:])


def attention_kernel(where_ref, q_ref, *rest):
    pieces, (mine_ref, other_ref, s_ref) = rest[:-3], rest[-3:]
    z, y, c = where_ref[0], where_ref[1], where_ref[2]
    nz = where_ref[3]
    del nz
    r = pl.program_id(0)
    yq = lax.rem(y - r + 4, 4)
    rows = q_ref.shape[1]
    tok = rows // 2
    row = lax.broadcasted_iota(jnp.int32, (rows, tok), 0)
    col = lax.broadcasted_iota(jnp.int32, (rows, tok), 1)
    first = row < tok
    qpos = yq * rows + jnp.where(first, row + c * tok, row - tok + (1 - c) * tok)
    kpos = y * rows + c * tok + col
    mask = kpos <= qpos
    lanes = 128
    sources = [0, -1, -2, -3, 1, 2, 3, 4, 4]
    biases, starts, at = [], [], 0
    for ref, step in zip(pieces, sources):
        source = lax.rem(z + step + 8, 8)
        biases.append(jnp.where(source <= z, 0.0, NEG).astype(jnp.float32))
        starts.append(at)
        at += ref.shape[0]
    out = []
    lse = []
    for m in range(2):
        q = q_ref[0, :, m * HEAD : (m + 1) * HEAD]
        high = jnp.full((rows, lanes), FLOOR, jnp.float32)
        for n, ref in enumerate(pieces):
            keys = ref.shape[0]
            s = dot_nt(q, ref[:, m * HEAD : (m + 1) * HEAD])
            if n == 0:
                s = jnp.where(mask, s, NEG)
            s_ref[:, starts[n] : starts[n] + keys] = s
            top = s[:, :lanes]
            for k in range(lanes, keys, lanes):
                top = jnp.maximum(top, s[:, k : k + lanes])
            high = jnp.maximum(high, top * SCALE2 + biases[n])
        high = jnp.max(high, axis=1, keepdims=True)
        total = jnp.zeros((rows, lanes), jnp.float32)
        acc = jnp.zeros((rows, 2 * HEAD), jnp.float32)
        for n, ref in enumerate(pieces):
            keys = ref.shape[0]
            p = jnp.exp2(s_ref[:, starts[n] : starts[n] + keys] * SCALE2 - (high - biases[n]))
            for k in range(0, keys, lanes):
                total = total + p[:, k : k + lanes]
            acc = acc + dot_nn(p.astype(jnp.bfloat16), ref[:, 2 * HEAD :])
        total = jnp.sum(total, axis=1, keepdims=True)
        out.append((acc * (1.0 / jnp.maximum(total, 1e-30))).astype(jnp.bfloat16))
        lse.append(jnp.where(total > 0.0, high + jnp.log2(jnp.maximum(total, 1e-30)), NEG))
    for h, ref in enumerate((mine_ref, other_ref)):
        part = slice(h * tok, (h + 1) * tok)
        ref[0, :tok, : 2 * HEAD] = out[0][part]
        ref[0, :tok, 2 * HEAD :] = out[1][part]
        ref[0, tok:, :] = stat_rows([lse[0][part], lse[1][part]])


def attention(where, q, pieces):
    count, rows, _ = q.shape
    tok = rows // 2
    keys = sum(p.shape[0] for p in pieces)
    width = pieces[0].shape[1]
    block = jax.ShapeDtypeStruct((count, tok + STAT, width), jnp.bfloat16)
    flops = 2 * 2 * count * rows * keys * 3 * HEAD
    return pl.pallas_call(
        attention_kernel,
        grid=(count,),
        out_shape=(block, block),
        in_specs=[SMEM, pl.BlockSpec((1, rows, 2 * HEAD), lambda r: (r, 0, 0))]
        + [pl.BlockSpec(p.shape, lambda r: (0, 0)) for p in pieces],
        out_specs=[pl.BlockSpec((1, tok + STAT, width), lambda r: (r, 0, 0))] * 2,
        scratch_shapes=[pltpu.VMEM((rows, keys), jnp.float32)],
        compiler_params=pltpu.CompilerParams(vmem_limit_bytes=40 * 1024 * 1024),
        cost_estimate=pl.CostEstimate(
            flops=flops, bytes_accessed=6 * 1024 * 1024, transcendentals=2 * count * rows * keys
        ),
        name="attention_partials",
    )(where, q, *pieces)


def merged(blocks):
    tok = blocks[0].shape[0] - STAT
    stats = [read_stats(b) for b in blocks]
    outs, lses = [], []
    for m in range(2):
        top = stats[0][m]
        for s in stats[1:]:
            top = jnp.maximum(top, s[m])
        weights = [jnp.exp2(s[m] - top) for s in stats]
        total = sum(weights[1:], weights[0])
        acc = None
        for w, b in zip(weights, blocks):
            term = w * b[:tok, m * 2 * HEAD : (m + 1) * 2 * HEAD].astype(jnp.float32)
            acc = term if acc is None else acc + term
        outs.append(acc / total)
        lses.append(top + jnp.log2(total))
    return outs, lses


def merge_kernel(a_ref, b_ref, *out_refs):
    for r, ref in enumerate(out_refs):
        tok = ref.shape[0] - STAT
        outs, lses = merged([a_ref[r], b_ref[r]])
        ref[:tok, : 2 * HEAD] = outs[0].astype(jnp.bfloat16)
        ref[:tok, 2 * HEAD :] = outs[1].astype(jnp.bfloat16)
        ref[tok:, :] = stat_rows(lses)


def merge_cores(a, b):
    count, rows, width = a.shape
    return pl.pallas_call(
        merge_kernel,
        out_shape=(jax.ShapeDtypeStruct((rows, width), jnp.bfloat16),) * count,
        in_specs=[VMEM, VMEM],
        out_specs=(VMEM,) * count,
        cost_estimate=pl.CostEstimate(flops=4_000_000_000, bytes_accessed=3 * a.size * 2, transcendentals=0),
        name="merge_cores",
    )(a, b)


def finish_kernel(lam_ref, gain_ref, *refs):
    blocks, out_ref = [ref[...] for ref in refs[:-1]], refs[-1]
    outs, _ = merged(blocks)
    mixed = outs[0] - lam_ref[0] * outs[1]
    mean = jnp.mean(mixed * mixed, axis=1, keepdims=True)
    out_ref[...] = (mixed * lax.rsqrt(mean + EPS) * gain_ref[...] * 0.8).astype(jnp.bfloat16)


def finish(lam, gain, blocks):
    tok = blocks[0].shape[0] - STAT
    return pl.pallas_call(
        finish_kernel,
        out_shape=jax.ShapeDtypeStruct((tok, 2 * HEAD), jnp.bfloat16),
        in_specs=[SMEM] + [VMEM] * (1 + len(blocks)),
        out_specs=VMEM,
        cost_estimate=pl.CostEstimate(flops=4_000_000_000, bytes_accessed=2_000_000, transcendentals=0),
        name="finish_heads",
    )(lam, gain.reshape(1, -1), *blocks)


def project_kernel(where_ref, gain_ref, *refs):
    att, own_w, near_w, far_w, res = refs[:4], refs[4], refs[5:8], refs[8:11], refs[11:15]
    own_ref, normed_ref, sum_ref = refs[15:]
    x, c = where_ref[4], where_ref[2]
    block = res[0].shape[1]
    half = near_w[0].shape[1]
    for s in range(4):
        at = pl.multiple_of(lax.rem(x - s + 4, 4) * block, block)
        sum_ref[:, pl.ds(at, block)] = res[s][...].astype(jnp.float32)
    square = jnp.zeros((own_ref.shape[0], 1), jnp.float32)
    for h, group in ((c, near_w), (1 - c, far_w)):
        for k in range(0, half, block):
            at = pl.multiple_of(h * half + k, block)
            cols = pl.ds(at, block)
            acc = dot_nn(att[0][...], own_w[:, cols]).astype(jnp.bfloat16).astype(jnp.float32)
            for s in range(3):
                part = dot_nn(att[s + 1][...], group[s][:, k : k + block])
                acc = acc + part.astype(jnp.bfloat16).astype(jnp.float32)
            resid = (sum_ref[:, cols] + acc).astype(jnp.bfloat16).astype(jnp.float32)
            sum_ref[:, cols] = resid
            square = square + jnp.sum(resid * resid, axis=1, keepdims=True)
    width = sum_ref.shape[1]
    scale = lax.rsqrt(square * (1.0 / width) + EPS)
    own_ref[...] = sum_ref[:, pl.ds(pl.multiple_of(x * block, block), block)].astype(jnp.bfloat16)
    normed_ref[...] = (sum_ref[...] * scale * gain_ref[...]).astype(jnp.bfloat16)


def project(where, gain, att, own_w, near_w, far_w, res):
    tok, block = res[0].shape
    width = own_w.shape[1]
    return pl.pallas_call(
        project_kernel,
        out_shape=(
            jax.ShapeDtypeStruct((tok, block), jnp.bfloat16),
            jax.ShapeDtypeStruct((tok, width), jnp.bfloat16),
        ),
        in_specs=[SMEM] + [VMEM] * 16,
        out_specs=(VMEM, VMEM),
        scratch_shapes=[pltpu.VMEM((tok, width), jnp.float32)],
        compiler_params=pltpu.CompilerParams(vmem_limit_bytes=40 * 1024 * 1024),
        cost_estimate=pl.CostEstimate(flops=2_000_000_000, bytes_accessed=8_000_000, transcendentals=0),
        name="project_norm",
    )(where, gain.reshape(1, -1), *att, own_w, *near_w, *far_w, *res)


def per_device(q1, q2, k1, k2, v, lam, hgain, ow, res, ngain, gw, uw, dw):
    z, y, c, x = (lax.axis_index(n).astype(jnp.int32) for n in ("z", "y", "c", "x"))
    where = jnp.stack([z, y, c, jnp.int32(8), x])

    hidden_here = gw.shape[1]
    both = jnp.concatenate([gw, uw, dw.T], axis=1)
    full = lax.all_gather(both, ("z", "y", "c"), axis=0, tiled=True)

    kv = jnp.concatenate([k1, k2, v], axis=1)
    tok = kv.shape[0]
    up, down = [kv], [kv]
    for _ in range(3):
        up.append(shift(up[-1], "z", 8, 1))
        down.append(shift(down[-1], "z", 8, -1))
    half_up = shift(up[3][: tok // 2], "z", 8, 1)
    half_down = shift(down[3][tok // 2 :], "z", 8, -1)
    pieces = [kv, *up[1:], *down[1:], half_up, half_down]

    q = jnp.concatenate([q1, q2], axis=1)
    pair = jnp.concatenate([q, shift(q, "c", 2, 1)], axis=0)
    queries = jnp.stack([pair] + [shift(pair, "y", 4, s) for s in range(1, 4)])

    half = ow.shape[1] // 2
    ow_half = lax.dynamic_slice_in_dim(ow, c * half, half, 1)
    near = [shift(ow_half, "x", 4, s) for s in range(1, 4)]
    far = [shift(w, "c", 2, 1) for w in near]
    residual = [res] + [shift(res, "x", 4, s) for s in range(1, 4)]

    mine, other = attention(where, queries, pieces)
    theirs = shift(other, "c", 2, 1)
    blocks = merge_cores(mine, theirs)
    arrived = [blocks[0]] + [shift(blocks[s], "y", 4, -s) for s in range(1, 4)]
    attended = finish(lam, hgain, arrived)
    att = [attended] + [shift(attended, "x", 4, s) for s in range(1, 4)]
    own, normed = project(where, ngain, att, ow, near, far, residual)

    gate_act = jnp.dot(normed, full[:, :hidden_here], preferred_element_type=jnp.float32)
    up_act = jnp.dot(normed, full[:, hidden_here : 2 * hidden_here], preferred_element_type=jnp.float32)
    hidden = (jax.nn.silu(gate_act) * up_act).astype(jnp.bfloat16)
    partial = dot_nt(hidden, full[:, 2 * hidden_here :]).astype(jnp.bfloat16)
    width = res.shape[1]
    parts = [
        lax.dynamic_slice_in_dim(partial, lax.rem(x + s, 4) * width, width, 1) for s in range(4)
    ]
    total = own.astype(jnp.float32) + parts[0].astype(jnp.float32)
    for s in range(1, 4):
        total = total + shift(parts[s], "x", 4, s).astype(jnp.float32)
    return total.astype(jnp.bfloat16)


def solution(mesh):
    fine = Mesh(mesh.devices.reshape(8, 4, 2, 4), ("z", "y", "c", "x"))
    sp = ("z", "y", "c")
    in_specs = (P(sp, "x"),) * 5 + (
        P("x"),
        P("x"),
        P("x", None),
        P(sp, "x"),
        P(),
        P(sp, "x"),
        P(sp, "x"),
        P("x", sp),
    )
    return jax.shard_map(
        per_device, mesh=fine, in_specs=in_specs, out_specs=P(sp, "x"), check_vma=False
    )
```

```python
import functools
import math

import jax
import jax.numpy as jnp
from jax import lax
from jax.experimental import pallas as pl
from jax.experimental.pallas import tpu as pltpu
from jax.sharding import Mesh
from jax.sharding import PartitionSpec as P

HEAD = 128
EPS = 1e-06
NEG = -1e30
FLOOR = -1e20
SCALE2 = HEAD**-0.5 * math.log2(math.e)
STAT = 16


VMEM = pl.BlockSpec(memory_space=pltpu.VMEM)
SMEM = pl.BlockSpec(memory_space=pltpu.SMEM)


def shift(a, axis, count, by):
    return lax.ppermute(a, axis, [(i, (i + by) % count) for i in range(count)])


def dot_nt(a, b):
    return lax.dot_general(a, b, (((1,), (1,)), ((), ())), preferred_element_type=jnp.float32)


def dot_nn(a, b):
    return lax.dot_general(a, b, (((1,), (0,)), ((), ())), preferred_element_type=jnp.float32)


def eye(n):
    return lax.broadcasted_iota(jnp.int32, (n, n), 0) == lax.broadcasted_iota(jnp.int32, (n, n), 1)


def to_row(col):
    n = col.shape[0]
    return jnp.sum(jnp.where(eye(n), col, 0.0), axis=0, keepdims=True)


def to_col(row):
    n = row.shape[1]
    return jnp.sum(jnp.where(eye(n), row, 0.0), axis=1, keepdims=True)


def stat_rows(lse_cols):
    row = jnp.concatenate([to_row(c) for c in lse_cols], axis=1)
    high = row.astype(jnp.bfloat16)
    rest = row - high.astype(jnp.float32)
    mid = rest.astype(jnp.bfloat16)
    low = (rest - mid.astype(jnp.float32)).astype(jnp.bfloat16)
    index = lax.broadcasted_iota(jnp.int32, (STAT, row.shape[1]), 0)
    zero = jnp.zeros_like(row)
    picked = jnp.where(
        index == 0,
        high.astype(jnp.float32),
        jnp.where(index == 1, mid.astype(jnp.float32), jnp.where(index == 2, low.astype(jnp.float32), zero)),
    )
    return picked.astype(jnp.bfloat16)


def read_stats(block, m):
    rows = block.shape[0] - STAT
    half = block.shape[1] // 2
    stats = block[rows:, m * half : (m + 1) * half].astype(jnp.float32)
    return to_col(jnp.sum(stats, axis=0, keepdims=True))


def attention_kernel(steps, carried, where_ref, q_ref, other_q_ref, *rest):
    pieces, rest = rest[: len(steps)], rest[len(steps) :]
    before, (mine_ref, other_ref, s_ref) = rest[:-3], rest[-3:]
    z, y, c = where_ref[0], where_ref[1], where_ref[2]
    r = pl.program_id(0)
    yq = lax.rem(y - r + 4, 4)
    tok = q_ref.shape[1]
    rows = 2 * tok
    lanes = 128
    biases, starts, at = [], [], 0
    for ref, step in zip(pieces, steps):
        source = lax.rem(z + step + 8, 8)
        biases.append(jnp.where(source <= z, 0.0, NEG).astype(jnp.float32))
        starts.append(at)
        at += ref.shape[0]
    out = []
    lse = []
    for m in range(2):
        heads = slice(m * HEAD, (m + 1) * HEAD)
        q = jnp.concatenate([q_ref[0, :, heads], other_q_ref[0, :, heads]], axis=0)
        high = jnp.full((rows, lanes), FLOOR, jnp.float32)
        for n, ref in enumerate(pieces):
            keys = ref.shape[0]
            s = dot_nt(q, ref[:, heads])
            if steps[n] == 0:
                row = lax.broadcasted_iota(jnp.int32, (rows, keys), 0)
                col = lax.broadcasted_iota(jnp.int32, (rows, keys), 1)
                qpos = yq * rows + jnp.where(row < tok, row + c * tok, row - tok + (1 - c) * tok)
                s = jnp.where(y * rows + c * tok + col <= qpos, s, NEG)
            s_ref[:, starts[n] : starts[n] + keys] = s
            top = s[:, :lanes]
            for k in range(lanes, keys, lanes):
                top = jnp.maximum(top, s[:, k : k + lanes])
            high = jnp.maximum(high, top * SCALE2 + biases[n])
        high = jnp.max(high, axis=1, keepdims=True)
        total = jnp.zeros((rows, lanes), jnp.float32)
        acc = jnp.zeros((rows, 2 * HEAD), jnp.float32)
        for n, ref in enumerate(pieces):
            keys = ref.shape[0]
            p = jnp.exp2(s_ref[:, starts[n] : starts[n] + keys] * SCALE2 - (high - biases[n]))
            for k in range(0, keys, lanes):
                total = total + p[:, k : k + lanes]
            acc = acc + dot_nn(p.astype(jnp.bfloat16), ref[:, 2 * HEAD :])
        total = jnp.sum(total, axis=1, keepdims=True)
        if carried:
            stats = jnp.concatenate([read_stats(ref[0], m) for ref in before], axis=0)
            old = jnp.concatenate(
                [ref[0, :tok, m * 2 * HEAD : (m + 1) * 2 * HEAD] for ref in before], axis=0
            )
            now = jnp.where(total > 0.0, high + jnp.log2(jnp.maximum(total, 1e-30)), NEG)
            top = jnp.maximum(stats, now)
            w_old, w_now = jnp.exp2(stats - top), jnp.exp2(now - top)
            both = w_old + w_now
            scale_now = w_now / (jnp.maximum(total, 1e-30) * both)
            out.append((acc * scale_now + old.astype(jnp.float32) * (w_old / both)).astype(jnp.bfloat16))
            lse.append(top + jnp.log2(both))
        else:
            out.append((acc * (1.0 / jnp.maximum(total, 1e-30))).astype(jnp.bfloat16))
            lse.append(jnp.where(total > 0.0, high + jnp.log2(jnp.maximum(total, 1e-30)), NEG))
    for h, ref in enumerate((mine_ref, other_ref)):
        part = slice(h * tok, (h + 1) * tok)
        ref[0, :tok, : 2 * HEAD] = out[0][part]
        ref[0, :tok, 2 * HEAD :] = out[1][part]
        ref[0, tok:, :] = stat_rows([lse[0][part], lse[1][part]])


def attention(where, q, other_q, pieces, steps, before):
    count, tok, _ = q.shape
    rows = 2 * tok
    keys = sum(p.shape[0] for p in pieces)
    width = pieces[0].shape[1]
    block = jax.ShapeDtypeStruct((count, tok + STAT, width), jnp.bfloat16)
    flops = 2 * 2 * count * rows * keys * 3 * HEAD
    spec = pl.BlockSpec((1, tok + STAT, width), lambda r: (r, 0, 0))
    return pl.pallas_call(
        functools.partial(attention_kernel, steps, bool(before)),
        grid=(count,),
        out_shape=(block, block),
        in_specs=[SMEM]
        + [pl.BlockSpec((1, tok, 2 * HEAD), lambda r: (r, 0, 0))] * 2
        + [pl.BlockSpec(p.shape, lambda r: (0, 0)) for p in pieces]
        + [spec] * len(before),
        out_specs=[spec, spec],
        scratch_shapes=[pltpu.VMEM((rows, keys), jnp.float32)],
        compiler_params=pltpu.CompilerParams(vmem_limit_bytes=32 * 1024 * 1024),
        cost_estimate=pl.CostEstimate(
            flops=flops, bytes_accessed=4 * 1024 * 1024, transcendentals=2 * count * rows * keys
        ),
    )(where, q, other_q, *pieces, *before)


def merged(blocks):
    tok = blocks[0].shape[0] - STAT
    stats = [[read_stats(b, m) for m in range(2)] for b in blocks]
    outs, lses = [], []
    for m in range(2):
        top = stats[0][m]
        for s in stats[1:]:
            top = jnp.maximum(top, s[m])
        weights = [jnp.exp2(s[m] - top) for s in stats]
        total = sum(weights[1:], weights[0])
        acc = None
        for w, b in zip(weights, blocks):
            term = w * b[:tok, m * 2 * HEAD : (m + 1) * 2 * HEAD].astype(jnp.float32)
            acc = term if acc is None else acc + term
        outs.append(acc / total)
        lses.append(top + jnp.log2(total))
    return outs, lses


def merge_kernel(a_ref, b_ref, *out_refs):
    for r, ref in enumerate(out_refs):
        tok = ref.shape[0] - STAT
        outs, lses = merged([a_ref[r], b_ref[r]])
        ref[:tok, : 2 * HEAD] = outs[0].astype(jnp.bfloat16)
        ref[:tok, 2 * HEAD :] = outs[1].astype(jnp.bfloat16)
        ref[tok:, :] = stat_rows(lses)


def merge_cores(a, b):
    count, rows, width = a.shape
    return pl.pallas_call(
        merge_kernel,
        out_shape=(jax.ShapeDtypeStruct((rows, width), jnp.bfloat16),) * count,
        in_specs=[VMEM, VMEM],
        out_specs=(VMEM,) * count,
        cost_estimate=pl.CostEstimate(flops=4_000_000_000, bytes_accessed=3 * a.size * 2, transcendentals=0),
        name="merge_cores",
    )(a, b)


def finish_kernel(lam_ref, gain_ref, *refs):
    blocks, out_ref = [ref[...] for ref in refs[:-1]], refs[-1]
    outs, _ = merged(blocks)
    mixed = outs[0] - lam_ref[0] * outs[1]
    mean = jnp.mean(mixed * mixed, axis=1, keepdims=True)
    out_ref[...] = (mixed * lax.rsqrt(mean + EPS) * gain_ref[...] * 0.8).astype(jnp.bfloat16)


def finish(lam, gain, blocks):
    tok = blocks[0].shape[0] - STAT
    return pl.pallas_call(
        finish_kernel,
        out_shape=jax.ShapeDtypeStruct((tok, 2 * HEAD), jnp.bfloat16),
        in_specs=[SMEM] + [VMEM] * (1 + len(blocks)),
        out_specs=VMEM,
        cost_estimate=pl.CostEstimate(flops=4_000_000_000, bytes_accessed=2_000_000, transcendentals=0),
        name="finish_heads",
    )(lam, gain.reshape(1, -1), *blocks)


def project_kernel(where_ref, gain_ref, *refs):
    att, (ow_ref, res_ref), extra = refs[:4], refs[4:6], refs[6:10]
    own_ref, normed_ref, sum_ref = refs[10:]
    x = where_ref[3]
    tok, block = res_ref.shape
    width = ow_ref.shape[1]
    half = tok // 2
    left, low, high, right = extra

    def at(s):
        return pl.ds(pl.multiple_of(lax.rem(x - s + 4, 4) * block, block), block)

    sum_ref[:, at(0)] = res_ref[...].astype(jnp.float32)
    sum_ref[:, at(1)] = left[:, width:].astype(jnp.float32)
    sum_ref[:half, at(2)] = low[:, width:].astype(jnp.float32)
    sum_ref[half:, at(2)] = high[:, width:].astype(jnp.float32)
    sum_ref[:, at(3)] = right[:, width:].astype(jnp.float32)
    square = jnp.zeros((tok, 1), jnp.float32)
    for k in range(0, width, block):
        cols = slice(k, k + block)
        acc = sum_ref[:, cols]
        parts = (
            dot_nn(att[0][...], ow_ref[:, cols]),
            dot_nn(att[1][...], left[:, cols]),
            dot_nn(att[2][:, :half], low[:, cols]) + dot_nn(att[2][:, half:], high[:, cols]),
            dot_nn(att[3][...], right[:, cols]),
        )
        total = None
        for part in parts:
            part = part.astype(jnp.bfloat16).astype(jnp.float32)
            total = part if total is None else total + part
        resid = (acc + total).astype(jnp.bfloat16).astype(jnp.float32)
        sum_ref[:, cols] = resid
        square = square + jnp.sum(resid * resid, axis=1, keepdims=True)
    scale = lax.rsqrt(square * (1.0 / width) + EPS)
    own_ref[...] = sum_ref[:, at(0)].astype(jnp.bfloat16)
    normed_ref[...] = (sum_ref[...] * scale * gain_ref[...]).astype(jnp.bfloat16)


def project(where, gain, att, ow, res, extra):
    tok, block = res.shape
    width = ow.shape[1]
    return pl.pallas_call(
        project_kernel,
        out_shape=(
            jax.ShapeDtypeStruct((tok, block), jnp.bfloat16),
            jax.ShapeDtypeStruct((tok, width), jnp.bfloat16),
        ),
        in_specs=[SMEM] + [VMEM] * 11,
        out_specs=(VMEM, VMEM),
        scratch_shapes=[pltpu.VMEM((tok, width), jnp.float32)],
        compiler_params=pltpu.CompilerParams(vmem_limit_bytes=32 * 1024 * 1024),
        cost_estimate=pl.CostEstimate(flops=2_000_000_000, bytes_accessed=8_000_000, transcendentals=0),
        name="project_norm",
    )(where, gain.reshape(1, -1), *att, ow, res, *extra)


def mixer_kernel(where_ref, normed_ref, full_ref, lo_ref, hi_ref, one_ref, three_ref, here_ref, w_ref, d_ref, h_ref, sems):
    count, _, width = w_ref.shape
    _, block, units = d_ref.shape
    lane = width // 2
    half = lo_ref.shape[0]

    def copies(j):
        at = pl.multiple_of(j * lane, lane)
        return [
            pltpu.make_async_copy(
                full_ref.at[:, pl.ds(at + n * units, lane)],
                w_ref.at[j, :, pl.ds(n * lane, lane)],
                sems.at[n, j],
            )
            for n in range(2)
        ]

    def down_copy(n, s):
        row = pl.multiple_of(lax.rem(where_ref[3] + s, 4) * block, block)
        return pltpu.make_async_copy(
            full_ref.at[pl.ds(row, block), pl.ds(2 * units, units)], d_ref.at[n], sems.at[0, count + n]
        )

    @pl.loop(0, count)
    def _(j):
        for c in copies(j):
            c.start()

    ahead = (2, 1, 3, 0)
    for n, s in enumerate(ahead):
        down_copy(n, s).start()

    @pl.loop(0, count)
    def _(j):
        for c in copies(j):
            c.wait()
        both = dot_nn(normed_ref[...], w_ref[j])
        gate, up = both[:, :lane], both[:, lane:]
        cols = pl.ds(pl.multiple_of(j * lane, lane), lane)
        h_ref[:, cols] = (gate / (1.0 + jnp.exp(-gate)) * up).astype(jnp.bfloat16)

    for n, s in enumerate(ahead):
        down_copy(n, s).wait()
    two = dot_nt(h_ref[...], d_ref[0]).astype(jnp.bfloat16)
    lo_ref[...] = two[:half]
    hi_ref[...] = two[half:]
    for n, ref in enumerate((one_ref, three_ref, here_ref)):
        ref[...] = dot_nt(h_ref[...], d_ref[n + 1]).astype(jnp.bfloat16)


def mixer(where, normed, full, block):
    tok, width = normed.shape
    units = full.shape[1] // 3
    lane = 128
    count = units // lane
    whole = jax.ShapeDtypeStruct((tok, block), jnp.bfloat16)
    part = jax.ShapeDtypeStruct((tok // 2, block), jnp.bfloat16)
    return pl.pallas_call(
        mixer_kernel,
        out_shape=(part, part, whole, whole, whole),
        in_specs=[SMEM, VMEM, pl.BlockSpec(memory_space=pl.ANY)],
        out_specs=(VMEM,) * 5,
        scratch_shapes=[
            pltpu.VMEM((count, width, 2 * lane), jnp.bfloat16),
            pltpu.VMEM((4, block, units), jnp.bfloat16),
            pltpu.VMEM((tok, units), jnp.bfloat16),
            pltpu.SemaphoreType.DMA((2, count + 4)),
        ],
        compiler_params=pltpu.CompilerParams(vmem_limit_bytes=40 * 1024 * 1024),
        cost_estimate=pl.CostEstimate(
            flops=2 * tok * width * units * 3, bytes_accessed=18_000_000, transcendentals=tok * units
        ),
        name="mixer",
    )(where, normed, full)


def both_ways(a, axis, count):
    half = a.shape[0] // 2
    left = shift(a, axis, count, 1)
    right = shift(a, axis, count, -1)
    low = shift(left[:half], axis, count, 1)
    high = shift(right[half:], axis, count, -1)
    return [left, low, high, right]


def per_device(q1, q2, k1, k2, v, lam, hgain, ow, res, ngain, gw, uw, dw):
    z, y, c, x = (lax.axis_index(n).astype(jnp.int32) for n in ("z", "y", "c", "x"))
    where = jnp.stack([z, y, c, x])

    both = jnp.concatenate([gw, uw, dw.T], axis=1)
    full = lax.all_gather(both, ("z", "y", "c"), axis=0, tiled=True)

    q = jnp.concatenate([q1, q2], axis=1)
    seen = [q]
    for s in range(1, 4):
        seen.append(shift(q, "y", 4, s))
    queries = jnp.stack(seen)
    others = shift(queries, "c", 2, 1)

    kv = jnp.concatenate([k1, k2, v], axis=1)
    tok = kv.shape[0]
    up, down_ring = [kv], [kv]
    for _ in range(3):
        up.append(shift(up[-1], "z", 8, 1))
        down_ring.append(shift(down_ring[-1], "z", 8, -1))
    half_up = shift(up[3][: tok // 2], "z", 8, 1)
    half_down = shift(down_ring[3][tok // 2 :], "z", 8, -1)

    extra = both_ways(jnp.concatenate([ow, res], axis=1), "x", 4)

    part = attention(where, queries, others, [kv, up[1], down_ring[1], up[2], down_ring[2]], (0, -1, 1, -2, 2), ())
    mine, other = attention(where, queries, others, [up[3], down_ring[3], half_up, half_down], (-3, 3, 4, 4), part)
    theirs = shift(other, "c", 2, 1)
    blocks = merge_cores(mine, theirs)
    arrived = [blocks[0]] + [shift(blocks[s], "y", 4, -s) for s in range(1, 4)]
    attended = finish(lam, hgain, arrived)
    att = [attended] + [shift(attended, "x", 4, s) for s in range(1, 4)]
    own, normed = project(where, ngain, att, ow, res, extra)

    width = res.shape[1]
    lo, hi, one, three, here = mixer(where, normed, full, width)
    half = tok // 2

    def wide(a):
        return a.astype(jnp.float32)

    from_left = shift(lo, "x", 4, 1)
    from_right = shift(hi, "x", 4, -1)
    left_hi = shift(one[half:], "x", 4, 1)
    right_lo = shift(three[:half], "x", 4, -1)
    left_lo = shift((wide(one[:half]) + wide(from_left)).astype(jnp.bfloat16), "x", 4, 1)
    right_hi = shift((wide(three[half:]) + wide(from_right)).astype(jnp.bfloat16), "x", 4, -1)
    near = wide(own) + wide(here)
    first = near[:half] + wide(right_lo) + wide(left_lo)
    second = near[half:] + wide(left_hi) + wide(right_hi)
    return jnp.concatenate([first, second], axis=0).astype(jnp.bfloat16)


def solution(mesh):
    fine = Mesh(mesh.devices.reshape(8, 4, 2, 4), ("z", "y", "c", "x"))
    sp = ("z", "y", "c")
    in_specs = (P(sp, "x"),) * 5 + (
        P("x"),
        P("x"),
        P("x", None),
        P(sp, "x"),
        P(),
        P(sp, "x"),
        P(sp, "x"),
        P("x", sp),
    )

    return jax.shard_map(per_device, mesh=fine, in_specs=in_specs, out_specs=P(sp, "x"), check_vma=False)
```

```python
import functools
import math

import jax
import jax.numpy as jnp
from jax import lax
from jax.experimental import pallas as pl
from jax.experimental.pallas import tpu as pltpu
from jax.sharding import Mesh
from jax.sharding import PartitionSpec as P

HEAD = 128
EPS = 1e-06
NEG = -1e30
FLOOR = -1e20
SCALE2 = HEAD**-0.5 * math.log2(math.e)
STAT = 16


VMEM = pl.BlockSpec(memory_space=pltpu.VMEM)
SMEM = pl.BlockSpec(memory_space=pltpu.SMEM)


def shift(a, axis, count, by):
    return lax.ppermute(a, axis, [(i, (i + by) % count) for i in range(count)])


def dot_nt(a, b):
    return lax.dot_general(a, b, (((1,), (1,)), ((), ())), preferred_element_type=jnp.float32)


def dot_nn(a, b):
    return lax.dot_general(a, b, (((1,), (0,)), ((), ())), preferred_element_type=jnp.float32)


def eye(n):
    return lax.broadcasted_iota(jnp.int32, (n, n), 0) == lax.broadcasted_iota(jnp.int32, (n, n), 1)


def to_row(col):
    n = col.shape[0]
    return jnp.sum(jnp.where(eye(n), col, 0.0), axis=0, keepdims=True)


def to_col(row):
    n = row.shape[1]
    return jnp.sum(jnp.where(eye(n), row, 0.0), axis=1, keepdims=True)


def stat_rows(lse_cols):
    row = jnp.concatenate([to_row(c) for c in lse_cols], axis=1)
    high = row.astype(jnp.bfloat16)
    rest = row - high.astype(jnp.float32)
    mid = rest.astype(jnp.bfloat16)
    low = (rest - mid.astype(jnp.float32)).astype(jnp.bfloat16)
    index = lax.broadcasted_iota(jnp.int32, (STAT, row.shape[1]), 0)
    zero = jnp.zeros_like(row)
    picked = jnp.where(
        index == 0,
        high.astype(jnp.float32),
        jnp.where(index == 1, mid.astype(jnp.float32), jnp.where(index == 2, low.astype(jnp.float32), zero)),
    )
    return picked.astype(jnp.bfloat16)


def read_stats(block, m):
    rows = block.shape[0] - STAT
    half = block.shape[1] // 2
    stats = block[rows:, m * half : (m + 1) * half].astype(jnp.float32)
    return to_col(jnp.sum(stats, axis=0, keepdims=True))


def attention_kernel(steps, carried, where_ref, q_ref, other_q_ref, *rest):
    pieces, rest = rest[: len(steps)], rest[len(steps) :]
    before, (mine_ref, other_ref, s_ref) = rest[:-3], rest[-3:]
    z, y, c = where_ref[0], where_ref[1], where_ref[2]
    r = pl.program_id(0)
    yq = lax.rem(y - r + 4, 4)
    tok = q_ref.shape[1]
    rows = 2 * tok
    lanes = 128
    biases, starts, at = [], [], 0
    for ref, step in zip(pieces, steps):
        source = lax.rem(z + step + 8, 8)
        biases.append(jnp.where(source <= z, 0.0, NEG).astype(jnp.float32))
        starts.append(at)
        at += ref.shape[0]
    out = []
    lse = []
    for m in range(2):
        heads = slice(m * HEAD, (m + 1) * HEAD)
        q = jnp.concatenate([q_ref[0, :, heads], other_q_ref[0, :, heads]], axis=0)
        high = jnp.full((rows, lanes), FLOOR, jnp.float32)
        for n, ref in enumerate(pieces):
            keys = ref.shape[0]
            s = dot_nt(q, ref[:, heads])
            if steps[n] == 0:
                row = lax.broadcasted_iota(jnp.int32, (rows, keys), 0)
                col = lax.broadcasted_iota(jnp.int32, (rows, keys), 1)
                qpos = yq * rows + jnp.where(row < tok, row + c * tok, row - tok + (1 - c) * tok)
                s = jnp.where(y * rows + c * tok + col <= qpos, s, NEG)
            s_ref[:, starts[n] : starts[n] + keys] = s
            top = s[:, :lanes]
            for k in range(lanes, keys, lanes):
                top = jnp.maximum(top, s[:, k : k + lanes])
            high = jnp.maximum(high, top * SCALE2 + biases[n])
        high = jnp.max(high, axis=1, keepdims=True)
        total = jnp.zeros((rows, lanes), jnp.float32)
        acc = jnp.zeros((rows, 2 * HEAD), jnp.float32)
        for n, ref in enumerate(pieces):
            keys = ref.shape[0]
            p = jnp.exp2(s_ref[:, starts[n] : starts[n] + keys] * SCALE2 - (high - biases[n]))
            for k in range(0, keys, lanes):
                total = total + p[:, k : k + lanes]
            acc = acc + dot_nn(p.astype(jnp.bfloat16), ref[:, 2 * HEAD :])
        total = jnp.sum(total, axis=1, keepdims=True)
        if carried:
            stats = jnp.concatenate([read_stats(ref[0], m) for ref in before], axis=0)
            old = jnp.concatenate(
                [ref[0, :tok, m * 2 * HEAD : (m + 1) * 2 * HEAD] for ref in before], axis=0
            )
            now = jnp.where(total > 0.0, high + jnp.log2(jnp.maximum(total, 1e-30)), NEG)
            top = jnp.maximum(stats, now)
            w_old, w_now = jnp.exp2(stats - top), jnp.exp2(now - top)
            both = w_old + w_now
            scale_now = w_now / (jnp.maximum(total, 1e-30) * both)
            out.append((acc * scale_now + old.astype(jnp.float32) * (w_old / both)).astype(jnp.bfloat16))
            lse.append(top + jnp.log2(both))
        else:
            out.append((acc * (1.0 / jnp.maximum(total, 1e-30))).astype(jnp.bfloat16))
            lse.append(jnp.where(total > 0.0, high + jnp.log2(jnp.maximum(total, 1e-30)), NEG))
    for h, ref in enumerate((mine_ref, other_ref)):
        part = slice(h * tok, (h + 1) * tok)
        ref[0, :tok, : 2 * HEAD] = out[0][part]
        ref[0, :tok, 2 * HEAD :] = out[1][part]
        ref[0, tok:, :] = stat_rows([lse[0][part], lse[1][part]])


def attention(where, q, other_q, pieces, steps, before):
    count, tok, _ = q.shape
    rows = 2 * tok
    keys = sum(p.shape[0] for p in pieces)
    width = pieces[0].shape[1]
    block = jax.ShapeDtypeStruct((count, tok + STAT, width), jnp.bfloat16)
    flops = 2 * 2 * count * rows * keys * 3 * HEAD
    spec = pl.BlockSpec((1, tok + STAT, width), lambda r: (r, 0, 0))
    return pl.pallas_call(
        functools.partial(attention_kernel, steps, bool(before)),
        grid=(count,),
        out_shape=(block, block),
        in_specs=[SMEM]
        + [pl.BlockSpec((1, tok, 2 * HEAD), lambda r: (r, 0, 0))] * 2
        + [pl.BlockSpec(p.shape, lambda r: (0, 0)) for p in pieces]
        + [spec] * len(before),
        out_specs=[spec, spec],
        scratch_shapes=[pltpu.VMEM((rows, keys), jnp.float32)],
        compiler_params=pltpu.CompilerParams(vmem_limit_bytes=20 * 1024 * 1024),
        cost_estimate=pl.CostEstimate(
            flops=flops, bytes_accessed=4 * 1024 * 1024, transcendentals=2 * count * rows * keys
        ),
    )(where, q, other_q, *pieces, *before)


def merged(blocks):
    tok = blocks[0].shape[0] - STAT
    stats = [[read_stats(b, m) for m in range(2)] for b in blocks]
    outs, lses = [], []
    for m in range(2):
        top = stats[0][m]
        for s in stats[1:]:
            top = jnp.maximum(top, s[m])
        weights = [jnp.exp2(s[m] - top) for s in stats]
        total = sum(weights[1:], weights[0])
        acc = None
        for w, b in zip(weights, blocks):
            term = w * b[:tok, m * 2 * HEAD : (m + 1) * 2 * HEAD].astype(jnp.float32)
            acc = term if acc is None else acc + term
        outs.append(acc / total)
        lses.append(top + jnp.log2(total))
    return outs, lses


def merge_kernel(a_ref, b_ref, *out_refs):
    for r, ref in enumerate(out_refs):
        tok = ref.shape[0] - STAT
        outs, lses = merged([a_ref[r], b_ref[r]])
        ref[:tok, : 2 * HEAD] = outs[0].astype(jnp.bfloat16)
        ref[:tok, 2 * HEAD :] = outs[1].astype(jnp.bfloat16)
        ref[tok:, :] = stat_rows(lses)


def merge_cores(a, b):
    count, rows, width = a.shape
    return pl.pallas_call(
        merge_kernel,
        out_shape=(jax.ShapeDtypeStruct((rows, width), jnp.bfloat16),) * count,
        in_specs=[VMEM, VMEM],
        out_specs=(VMEM,) * count,
        compiler_params=pltpu.CompilerParams(vmem_limit_bytes=10 * 1024 * 1024),
        cost_estimate=pl.CostEstimate(flops=4_000_000_000, bytes_accessed=3 * a.size * 2, transcendentals=0),
        name="merge_cores",
    )(a, b)


def finish_kernel(lam_ref, gain_ref, *refs):
    blocks, out_ref = [ref[...] for ref in refs[:-1]], refs[-1]
    outs, _ = merged(blocks)
    mixed = outs[0] - lam_ref[0] * outs[1]
    mean = jnp.mean(mixed * mixed, axis=1, keepdims=True)
    out_ref[...] = (mixed * lax.rsqrt(mean + EPS) * gain_ref[...] * 0.8).astype(jnp.bfloat16)


def finish(lam, gain, blocks):
    tok = blocks[0].shape[0] - STAT
    return pl.pallas_call(
        finish_kernel,
        out_shape=jax.ShapeDtypeStruct((tok, 2 * HEAD), jnp.bfloat16),
        in_specs=[SMEM] + [VMEM] * (1 + len(blocks)),
        out_specs=VMEM,
        compiler_params=pltpu.CompilerParams(vmem_limit_bytes=8 * 1024 * 1024),
        cost_estimate=pl.CostEstimate(flops=4_000_000_000, bytes_accessed=2_000_000, transcendentals=0),
        name="finish_heads",
    )(lam, gain.reshape(1, -1), *blocks)


def project_kernel(where_ref, gain_ref, *refs):
    att, (ow_ref, res_ref), extra = refs[:4], refs[4:6], refs[6:12]
    own_ref, normed_ref, sum_ref = refs[12:]
    x = where_ref[3]
    tok, block = res_ref.shape
    width = ow_ref.shape[1]
    half = tok // 2

    def at(s):
        return pl.ds(pl.multiple_of(lax.rem(x - s + 4, 4) * block, block), block)

    sum_ref[:, at(0)] = res_ref[...].astype(jnp.float32)
    for s in range(3):
        sum_ref[:half, at(s + 1)] = extra[2 * s][:, width:].astype(jnp.float32)
        sum_ref[half:, at(s + 1)] = extra[2 * s + 1][:, width:].astype(jnp.float32)
    square = jnp.zeros((tok, 1), jnp.float32)
    for k in range(0, width, block):
        cols = slice(k, k + block)
        acc = sum_ref[:, cols]
        parts = [dot_nn(att[0][...], ow_ref[:, cols])]
        for s in range(3):
            low, high = extra[2 * s], extra[2 * s + 1]
            parts.append(
                dot_nn(att[s + 1][:, :half], low[:, cols]) + dot_nn(att[s + 1][:, half:], high[:, cols])
            )
        total = None
        for part in parts:
            part = part.astype(jnp.bfloat16).astype(jnp.float32)
            total = part if total is None else total + part
        resid = (acc + total).astype(jnp.bfloat16).astype(jnp.float32)
        sum_ref[:, cols] = resid
        square = square + jnp.sum(resid * resid, axis=1, keepdims=True)
    scale = lax.rsqrt(square * (1.0 / width) + EPS)
    own_ref[...] = sum_ref[:, at(0)].astype(jnp.bfloat16)
    normed_ref[...] = (sum_ref[...] * scale * gain_ref[...]).astype(jnp.bfloat16)


def project(where, gain, att, ow, res, extra):
    tok, block = res.shape
    width = ow.shape[1]
    return pl.pallas_call(
        project_kernel,
        out_shape=(
            jax.ShapeDtypeStruct((tok, block), jnp.bfloat16),
            jax.ShapeDtypeStruct((tok, width), jnp.bfloat16),
        ),
        in_specs=[SMEM] + [VMEM] * 13,
        out_specs=(VMEM, VMEM),
        scratch_shapes=[pltpu.VMEM((tok, width), jnp.float32)],
        compiler_params=pltpu.CompilerParams(vmem_limit_bytes=16 * 1024 * 1024),
        cost_estimate=pl.CostEstimate(flops=2_000_000_000, bytes_accessed=8_000_000, transcendentals=0),
        name="project_norm",
    )(where, gain.reshape(1, -1), *att, ow, res, *extra)


def mixer_kernel(
    where_ref, normed_ref, full_ref, plus_ref, minus_ref, one_ref, three_ref, here_ref, w_ref, d_ref, h_ref, sems
):
    count, _, width = w_ref.shape
    _, block, units = d_ref.shape
    lane = width // 2
    half = one_ref.shape[0]

    def copies(j):
        at = pl.multiple_of(j * lane, lane)
        return [
            pltpu.make_async_copy(
                full_ref.at[:, pl.ds(at + n * units, lane)],
                w_ref.at[j, :, pl.ds(n * lane, lane)],
                sems.at[n, j],
            )
            for n in range(2)
        ]

    def down_copy(n, s):
        row = pl.multiple_of(lax.rem(where_ref[3] + s, 4) * block, block)
        return pltpu.make_async_copy(
            full_ref.at[pl.ds(row, block), pl.ds(2 * units, units)], d_ref.at[n], sems.at[0, count + n]
        )

    @pl.loop(0, count)
    def _(j):
        for c in copies(j):
            c.start()

    ahead = (2, 1, 3, 0)
    for n, s in enumerate(ahead):
        down_copy(n, s).start()

    @pl.loop(0, count)
    def _(j):
        for c in copies(j):
            c.wait()
        both = dot_nn(normed_ref[...], w_ref[j])
        gate, up = both[:, :lane], both[:, lane:]
        cols = pl.ds(pl.multiple_of(j * lane, lane), lane)
        h_ref[:, cols] = (gate / (1.0 + jnp.exp(-gate)) * up).astype(jnp.bfloat16)

    for n, s in enumerate(ahead):
        down_copy(n, s).wait()
    two, one, three, here = (dot_nt(h_ref[...], d_ref[n]).astype(jnp.bfloat16) for n in range(4))
    plus_ref[:half] = two[:half]
    plus_ref[half:] = one[half:]
    minus_ref[:half] = two[half:]
    minus_ref[half:] = three[:half]
    one_ref[...] = one[:half]
    three_ref[...] = three[half:]
    here_ref[...] = here


def mixer(where, normed, full, block):
    tok, width = normed.shape
    units = full.shape[1] // 3
    lane = 128
    count = units // lane
    whole = jax.ShapeDtypeStruct((tok, block), jnp.bfloat16)
    part = jax.ShapeDtypeStruct((tok // 2, block), jnp.bfloat16)
    return pl.pallas_call(
        mixer_kernel,
        out_shape=(whole, whole, part, part, whole),
        in_specs=[SMEM, VMEM, pl.BlockSpec(memory_space=pl.ANY)],
        out_specs=(VMEM,) * 5,
        scratch_shapes=[
            pltpu.VMEM((count, width, 2 * lane), jnp.bfloat16),
            pltpu.VMEM((4, block, units), jnp.bfloat16),
            pltpu.VMEM((tok, units), jnp.bfloat16),
            pltpu.SemaphoreType.DMA((2, count + 4)),
        ],
        compiler_params=pltpu.CompilerParams(vmem_limit_bytes=48 * 1024 * 1024),
        cost_estimate=pl.CostEstimate(
            flops=2 * tok * width * units * 3, bytes_accessed=18_000_000, transcendentals=tok * units
        ),
        name="mixer",
    )(where, normed, full)


def both_ways(halves, axis, count):
    first, second = halves
    left = [shift(h, axis, count, 1) for h in halves]
    right = [shift(h, axis, count, -1) for h in (second, first)]
    low = shift(left[0], axis, count, 1)
    high = shift(right[0], axis, count, -1)
    return [left[0], left[1], low, high, right[1], right[0]]


def per_device(q1, q2, k1, k2, v, lam, hgain, ow, res, ngain, gw, uw, dw):
    z, y, c, x = (lax.axis_index(n).astype(jnp.int32) for n in ("z", "y", "c", "x"))
    where = jnp.stack([z, y, c, x])

    both = jnp.concatenate([gw, uw, dw.T], axis=1)
    full = lax.all_gather(both, ("z", "y", "c"), axis=0, tiled=True)

    q = jnp.concatenate([q1, q2], axis=1)
    seen = [q]
    for s in range(1, 4):
        seen.append(shift(q, "y", 4, s))
    queries = jnp.stack(seen)
    others = shift(queries, "c", 2, 1)

    kv = jnp.concatenate([k1, k2, v], axis=1)
    tok = kv.shape[0]
    up, down_ring = [kv], [kv]
    for _ in range(3):
        up.append(shift(up[-1], "z", 8, 1))
        down_ring.append(shift(down_ring[-1], "z", 8, -1))
    half_up = shift(up[3][: tok // 2], "z", 8, 1)
    half_down = shift(down_ring[3][tok // 2 :], "z", 8, -1)

    half = tok // 2
    extra = both_ways(
        [jnp.concatenate([ow[h : h + half], res[h : h + half]], axis=1) for h in (0, half)], "x", 4
    )

    part = attention(where, queries, others, [kv, up[1], down_ring[1], up[2], down_ring[2]], (0, -1, 1, -2, 2), ())
    mine, other = attention(where, queries, others, [up[3], down_ring[3], half_up, half_down], (-3, 3, 4, 4), part)
    theirs = shift(other, "c", 2, 1)
    blocks = merge_cores(mine, theirs)
    arrived = [blocks[0]] + [shift(blocks[s], "y", 4, -s) for s in range(1, 4)]
    attended = finish(lam, hgain, arrived)
    att = [attended] + [shift(attended, "x", 4, s) for s in range(1, 4)]
    own, normed = project(where, ngain, att, ow, res, extra)

    width = res.shape[1]
    plus, minus, one_lo, three_hi, here = mixer(where, normed, full, width)

    def wide(a):
        return a.astype(jnp.float32)

    plus = shift(plus, "x", 4, 1)
    minus = shift(minus, "x", 4, -1)
    left_lo = shift((wide(one_lo) + wide(plus[:half])).astype(jnp.bfloat16), "x", 4, 1)
    right_hi = shift((wide(three_hi) + wide(minus[:half])).astype(jnp.bfloat16), "x", 4, -1)
    near = wide(own) + wide(here)
    first = near[:half] + wide(minus[half:]) + wide(left_lo)
    second = near[half:] + wide(plus[half:]) + wide(right_hi)
    return jnp.concatenate([first, second], axis=0).astype(jnp.bfloat16)


def solution(mesh):
    fine = Mesh(mesh.devices.reshape(8, 4, 2, 4), ("z", "y", "c", "x"))
    sp = ("z", "y", "c")
    in_specs = (P(sp, "x"),) * 5 + (
        P("x"),
        P("x"),
        P("x", None),
        P(sp, "x"),
        P(),
        P(sp, "x"),
        P(sp, "x"),
        P("x", sp),
    )

    return jax.shard_map(per_device, mesh=fine, in_specs=in_specs, out_specs=P(sp, "x"), check_vma=False)
```

```python
import functools
import math

import jax
import jax.numpy as jnp
from jax import lax
from jax.experimental import pallas as pl
from jax.experimental.pallas import tpu as pltpu
from jax.sharding import Mesh
from jax.sharding import PartitionSpec as P

HEAD = 128
EPS = 1e-06
NEG = -1e30
FLOOR = -1e20
SCALE2 = HEAD**-0.5 * math.log2(math.e)
STAT = 16
AHEAD = 4


VMEM = pl.BlockSpec(memory_space=pltpu.VMEM)
SMEM = pl.BlockSpec(memory_space=pltpu.SMEM)


def shift(a, axis, count, by):
    return lax.ppermute(a, axis, [(i, (i + by) % count) for i in range(count)])


def dot_nt(a, b):
    return lax.dot_general(a, b, (((1,), (1,)), ((), ())), preferred_element_type=jnp.float32)


def dot_nn(a, b):
    return lax.dot_general(a, b, (((1,), (0,)), ((), ())), preferred_element_type=jnp.float32)


def eye(n):
    return lax.broadcasted_iota(jnp.int32, (n, n), 0) == lax.broadcasted_iota(jnp.int32, (n, n), 1)


def to_row(col):
    n = col.shape[0]
    return jnp.sum(jnp.where(eye(n), col, 0.0), axis=0, keepdims=True)


def to_col(row):
    n = row.shape[1]
    return jnp.sum(jnp.where(eye(n), row, 0.0), axis=1, keepdims=True)


def stat_rows(lse_cols):
    row = jnp.concatenate([to_row(c) for c in lse_cols], axis=1)
    high = row.astype(jnp.bfloat16)
    rest = row - high.astype(jnp.float32)
    mid = rest.astype(jnp.bfloat16)
    low = (rest - mid.astype(jnp.float32)).astype(jnp.bfloat16)
    index = lax.broadcasted_iota(jnp.int32, (STAT, row.shape[1]), 0)
    zero = jnp.zeros_like(row)
    picked = jnp.where(
        index == 0,
        high.astype(jnp.float32),
        jnp.where(index == 1, mid.astype(jnp.float32), jnp.where(index == 2, low.astype(jnp.float32), zero)),
    )
    return picked.astype(jnp.bfloat16)


def read_stats(block, m):
    rows = block.shape[0] - STAT
    half = block.shape[1] // 2
    stats = block[rows:, m * half : (m + 1) * half].astype(jnp.float32)
    return to_col(jnp.sum(stats, axis=0, keepdims=True))


def attention_kernel(steps, carried, where_ref, q_ref, other_q_ref, *rest):
    pieces, rest = rest[: len(steps)], rest[len(steps) :]
    before, (mine_ref, other_ref, s_ref) = rest[:-3], rest[-3:]
    z, y, c = where_ref[0], where_ref[1], where_ref[2]
    r = pl.program_id(0)
    yq = lax.rem(y - r + 4, 4)
    tok = q_ref.shape[1]
    rows = 2 * tok
    lanes = 128
    biases, starts, at = [], [], 0
    for ref, step in zip(pieces, steps):
        source = lax.rem(z + step + 8, 8)
        biases.append(jnp.where(source <= z, 0.0, NEG).astype(jnp.float32))
        starts.append(at)
        at += ref.shape[0]
    out = []
    lse = []
    for m in range(2):
        heads = slice(m * HEAD, (m + 1) * HEAD)
        q = jnp.concatenate([q_ref[0, :, heads], other_q_ref[0, :, heads]], axis=0)
        high = jnp.full((rows, lanes), FLOOR, jnp.float32)
        for n, ref in enumerate(pieces):
            keys = ref.shape[0]
            s = dot_nt(q, ref[:, heads])
            if steps[n] == 0:
                row = lax.broadcasted_iota(jnp.int32, (rows, keys), 0)
                col = lax.broadcasted_iota(jnp.int32, (rows, keys), 1)
                qpos = yq * rows + jnp.where(row < tok, row + c * tok, row - tok + (1 - c) * tok)
                s = jnp.where(y * rows + c * tok + col <= qpos, s, NEG)
            s_ref[:, starts[n] : starts[n] + keys] = s
            top = s[:, :lanes]
            for k in range(lanes, keys, lanes):
                top = jnp.maximum(top, s[:, k : k + lanes])
            high = jnp.maximum(high, top * SCALE2 + biases[n])
        high = jnp.max(high, axis=1, keepdims=True)
        total = jnp.zeros((rows, lanes), jnp.float32)
        acc = jnp.zeros((rows, 2 * HEAD), jnp.float32)
        for n, ref in enumerate(pieces):
            keys = ref.shape[0]
            p = jnp.exp2(s_ref[:, starts[n] : starts[n] + keys] * SCALE2 - (high - biases[n]))
            for k in range(0, keys, lanes):
                total = total + p[:, k : k + lanes]
            acc = acc + dot_nn(p.astype(jnp.bfloat16), ref[:, 2 * HEAD :])
        total = jnp.sum(total, axis=1, keepdims=True)
        if carried:
            stats = jnp.concatenate([read_stats(ref[0], m) for ref in before], axis=0)
            old = jnp.concatenate(
                [ref[0, :tok, m * 2 * HEAD : (m + 1) * 2 * HEAD] for ref in before], axis=0
            )
            now = jnp.where(total > 0.0, high + jnp.log2(jnp.maximum(total, 1e-30)), NEG)
            top = jnp.maximum(stats, now)
            w_old, w_now = jnp.exp2(stats - top), jnp.exp2(now - top)
            both = w_old + w_now
            scale_now = w_now / (jnp.maximum(total, 1e-30) * both)
            out.append((acc * scale_now + old.astype(jnp.float32) * (w_old / both)).astype(jnp.bfloat16))
            lse.append(top + jnp.log2(both))
        else:
            out.append((acc * (1.0 / jnp.maximum(total, 1e-30))).astype(jnp.bfloat16))
            lse.append(jnp.where(total > 0.0, high + jnp.log2(jnp.maximum(total, 1e-30)), NEG))
    for h, ref in enumerate((mine_ref, other_ref)):
        part = slice(h * tok, (h + 1) * tok)
        ref[0, :tok, : 2 * HEAD] = out[0][part]
        ref[0, :tok, 2 * HEAD :] = out[1][part]
        ref[0, tok:, :] = stat_rows([lse[0][part], lse[1][part]])


def attention(where, q, other_q, pieces, steps, before):
    count, tok, _ = q.shape
    rows = 2 * tok
    keys = sum(p.shape[0] for p in pieces)
    width = pieces[0].shape[1]
    block = jax.ShapeDtypeStruct((count, tok + STAT, width), jnp.bfloat16)
    flops = 2 * 2 * count * rows * keys * 3 * HEAD
    spec = pl.BlockSpec((1, tok + STAT, width), lambda r: (r, 0, 0))
    return pl.pallas_call(
        functools.partial(attention_kernel, steps, bool(before)),
        grid=(count,),
        out_shape=(block, block),
        in_specs=[SMEM]
        + [pl.BlockSpec((1, tok, 2 * HEAD), lambda r: (r, 0, 0))] * 2
        + [pl.BlockSpec(p.shape, lambda r: (0, 0)) for p in pieces]
        + [spec] * len(before),
        out_specs=[spec, spec],
        scratch_shapes=[pltpu.VMEM((rows, keys), jnp.float32)],
        compiler_params=pltpu.CompilerParams(vmem_limit_bytes=20 * 1024 * 1024),
        cost_estimate=pl.CostEstimate(
            flops=flops, bytes_accessed=4 * 1024 * 1024, transcendentals=2 * count * rows * keys
        ),
    )(where, q, other_q, *pieces, *before)


def merged(blocks):
    tok = blocks[0].shape[0] - STAT
    stats = [[read_stats(b, m) for m in range(2)] for b in blocks]
    outs, lses = [], []
    for m in range(2):
        top = stats[0][m]
        for s in stats[1:]:
            top = jnp.maximum(top, s[m])
        weights = [jnp.exp2(s[m] - top) for s in stats]
        total = sum(weights[1:], weights[0])
        acc = None
        for w, b in zip(weights, blocks):
            term = w * b[:tok, m * 2 * HEAD : (m + 1) * 2 * HEAD].astype(jnp.float32)
            acc = term if acc is None else acc + term
        outs.append(acc / total)
        lses.append(top + jnp.log2(total))
    return outs, lses


def merge_kernel(a_ref, b_ref, *out_refs):
    for r, ref in enumerate(out_refs):
        tok = ref.shape[0] - STAT
        outs, lses = merged([a_ref[r], b_ref[r]])
        ref[:tok, : 2 * HEAD] = outs[0].astype(jnp.bfloat16)
        ref[:tok, 2 * HEAD :] = outs[1].astype(jnp.bfloat16)
        ref[tok:, :] = stat_rows(lses)


def merge_cores(a, b):
    count, rows, width = a.shape
    return pl.pallas_call(
        merge_kernel,
        out_shape=(jax.ShapeDtypeStruct((rows, width), jnp.bfloat16),) * count,
        in_specs=[VMEM, VMEM],
        out_specs=(VMEM,) * count,
        compiler_params=pltpu.CompilerParams(vmem_limit_bytes=10 * 1024 * 1024),
        cost_estimate=pl.CostEstimate(flops=4_000_000_000, bytes_accessed=3 * a.size * 2, transcendentals=0),
        name="merge_cores",
    )(a, b)


def finish_kernel(lam_ref, gain_ref, *refs):
    blocks, out_ref = [ref[...] for ref in refs[:-1]], refs[-1]
    outs, _ = merged(blocks)
    mixed = outs[0] - lam_ref[0] * outs[1]
    mean = jnp.mean(mixed * mixed, axis=1, keepdims=True)
    out_ref[...] = (mixed * lax.rsqrt(mean + EPS) * gain_ref[...] * 0.8).astype(jnp.bfloat16)


def finish(lam, gain, blocks):
    tok = blocks[0].shape[0] - STAT
    return pl.pallas_call(
        finish_kernel,
        out_shape=jax.ShapeDtypeStruct((tok, 2 * HEAD), jnp.bfloat16),
        in_specs=[SMEM] + [VMEM] * (1 + len(blocks)),
        out_specs=VMEM,
        compiler_params=pltpu.CompilerParams(vmem_limit_bytes=8 * 1024 * 1024),
        cost_estimate=pl.CostEstimate(flops=4_000_000_000, bytes_accessed=2_000_000, transcendentals=0),
        name="finish_heads",
    )(lam, gain.reshape(1, -1), *blocks)


def project_kernel(where_ref, gain_ref, *refs):
    att, (ow_ref, res_ref), extra = refs[:4], refs[4:6], refs[6:12]
    own_ref, normed_ref, sum_ref = refs[12:]
    x = where_ref[3]
    tok, block = res_ref.shape
    width = ow_ref.shape[1]
    half = tok // 2

    def at(s):
        return pl.ds(pl.multiple_of(lax.rem(x - s + 4, 4) * block, block), block)

    sum_ref[:, at(0)] = res_ref[...].astype(jnp.float32)
    for s in range(3):
        sum_ref[:half, at(s + 1)] = extra[2 * s][:, width:].astype(jnp.float32)
        sum_ref[half:, at(s + 1)] = extra[2 * s + 1][:, width:].astype(jnp.float32)
    square = jnp.zeros((tok, 1), jnp.float32)
    for k in range(0, width, block):
        cols = slice(k, k + block)
        acc = sum_ref[:, cols]
        parts = [dot_nn(att[0][...], ow_ref[:, cols])]
        for s in range(3):
            low, high = extra[2 * s], extra[2 * s + 1]
            parts.append(
                dot_nn(att[s + 1][:, :half], low[:, cols]) + dot_nn(att[s + 1][:, half:], high[:, cols])
            )
        total = None
        for part in parts:
            part = part.astype(jnp.bfloat16).astype(jnp.float32)
            total = part if total is None else total + part
        resid = (acc + total).astype(jnp.bfloat16).astype(jnp.float32)
        sum_ref[:, cols] = resid
        square = square + jnp.sum(resid * resid, axis=1, keepdims=True)
    scale = lax.rsqrt(square * (1.0 / width) + EPS)
    own_ref[...] = sum_ref[:, at(0)].astype(jnp.bfloat16)
    normed_ref[...] = (sum_ref[...] * scale * gain_ref[...]).astype(jnp.bfloat16)


def project(where, gain, att, ow, res, extra):
    tok, block = res.shape
    width = ow.shape[1]
    return pl.pallas_call(
        project_kernel,
        out_shape=(
            jax.ShapeDtypeStruct((tok, block), jnp.bfloat16),
            jax.ShapeDtypeStruct((tok, width), jnp.bfloat16),
        ),
        in_specs=[SMEM] + [VMEM] * 13,
        out_specs=(VMEM, VMEM),
        scratch_shapes=[pltpu.VMEM((tok, width), jnp.float32)],
        compiler_params=pltpu.CompilerParams(vmem_limit_bytes=16 * 1024 * 1024),
        cost_estimate=pl.CostEstimate(flops=2_000_000_000, bytes_accessed=8_000_000, transcendentals=0),
        name="project_norm",
    )(where, gain.reshape(1, -1), *att, ow, res, *extra)


def mixer_kernel(where_ref, normed_ref, full_ref, lo_ref, hi_ref, one_ref, three_ref, here_ref, w_ref, d_ref, h_ref, sems):
    count, _, width = w_ref.shape
    _, block, units = d_ref.shape
    lane = width // 2
    half = lo_ref.shape[0]

    def copies(j):
        at = pl.multiple_of(j * lane, lane)
        return [
            pltpu.make_async_copy(
                full_ref.at[:, pl.ds(at + n * units, lane)],
                w_ref.at[j, :, pl.ds(n * lane, lane)],
                sems.at[n, j],
            )
            for n in range(2)
        ]

    def down_copy(n):
        row = pl.multiple_of(lax.rem(where_ref[3] + n, 4) * block, block)
        return pltpu.make_async_copy(
            full_ref.at[pl.ds(row, block), pl.ds(2 * units, units)], d_ref.at[n], sems.at[0, count + n]
        )

    for j in range(AHEAD):
        for c in copies(j):
            c.start()

    @pl.loop(0, count)
    def _(j):
        for c in copies(j):
            c.wait()

        @pl.when(j + AHEAD < count)
        def _():
            for c in copies(j + AHEAD):
                c.start()

        @pl.when(j + AHEAD >= count)
        def _():
            down_copy(j + AHEAD - count).start()

        both = dot_nn(normed_ref[...], w_ref[j])
        gate, up = both[:, :lane], both[:, lane:]
        cols = pl.ds(pl.multiple_of(j * lane, lane), lane)
        h_ref[:, cols] = (gate / (1.0 + jnp.exp(-gate)) * up).astype(jnp.bfloat16)

    for n in range(4):
        down_copy(n).wait()
    two = dot_nt(h_ref[...], d_ref[2]).astype(jnp.bfloat16)
    lo_ref[...] = two[:half]
    hi_ref[...] = two[half:]
    for n, ref in ((1, one_ref), (3, three_ref), (0, here_ref)):
        ref[...] = dot_nt(h_ref[...], d_ref[n]).astype(jnp.bfloat16)


def mixer(where, normed, full, block):
    tok, width = normed.shape
    units = full.shape[1] // 3
    lane = 128
    count = units // lane
    whole = jax.ShapeDtypeStruct((tok, block), jnp.bfloat16)
    part = jax.ShapeDtypeStruct((tok // 2, block), jnp.bfloat16)
    return pl.pallas_call(
        mixer_kernel,
        out_shape=(part, part, whole, whole, whole),
        in_specs=[SMEM, VMEM, pl.BlockSpec(memory_space=pl.ANY)],
        out_specs=(VMEM,) * 5,
        scratch_shapes=[
            pltpu.VMEM((count, width, 2 * lane), jnp.bfloat16),
            pltpu.VMEM((4, block, units), jnp.bfloat16),
            pltpu.VMEM((tok, units), jnp.bfloat16),
            pltpu.SemaphoreType.DMA((2, count + 4)),
        ],
        compiler_params=pltpu.CompilerParams(vmem_limit_bytes=48 * 1024 * 1024),
        cost_estimate=pl.CostEstimate(
            flops=2 * tok * width * units * 3, bytes_accessed=18_000_000, transcendentals=tok * units
        ),
        name="mixer",
    )(where, normed, full)


def both_ways(halves, axis, count):
    first, second = halves
    left = [shift(h, axis, count, 1) for h in halves]
    right = [shift(h, axis, count, -1) for h in (second, first)]
    low = shift(left[0], axis, count, 1)
    high = shift(right[0], axis, count, -1)
    return [left[0], left[1], low, high, right[1], right[0]]


def per_device(q1, q2, k1, k2, v, lam, hgain, ow, res, ngain, gw, uw, dw):
    z, y, c, x = (lax.axis_index(n).astype(jnp.int32) for n in ("z", "y", "c", "x"))
    where = jnp.stack([z, y, c, x])

    both = jnp.concatenate([gw, uw, dw.T], axis=1)
    full = lax.all_gather(both, ("z", "y", "c"), axis=0, tiled=True)

    q = jnp.concatenate([q1, q2], axis=1)
    seen = [q]
    for s in range(1, 4):
        seen.append(shift(q, "y", 4, s))
    queries = jnp.stack(seen)
    others = shift(queries, "c", 2, 1)

    kv = jnp.concatenate([k1, k2, v], axis=1)
    tok = kv.shape[0]
    up, down_ring = [kv], [kv]
    for _ in range(3):
        up.append(shift(up[-1], "z", 8, 1))
        down_ring.append(shift(down_ring[-1], "z", 8, -1))
    half_up = shift(up[3][: tok // 2], "z", 8, 1)
    half_down = shift(down_ring[3][tok // 2 :], "z", 8, -1)

    half = tok // 2
    extra = both_ways(
        [jnp.concatenate([ow[h : h + half], res[h : h + half]], axis=1) for h in (0, half)], "x", 4
    )

    part = attention(where, queries, others, [kv, up[1], down_ring[1], up[2], down_ring[2]], (0, -1, 1, -2, 2), ())
    mine, other = attention(where, queries, others, [up[3], down_ring[3], half_up, half_down], (-3, 3, 4, 4), part)
    theirs = shift(other, "c", 2, 1)
    blocks = merge_cores(mine, theirs)
    arrived = [blocks[0]] + [shift(blocks[s], "y", 4, -s) for s in range(1, 4)]
    attended = finish(lam, hgain, arrived)
    att = [attended] + [shift(attended, "x", 4, s) for s in range(1, 4)]
    own, normed = project(where, ngain, att, ow, res, extra)

    width = res.shape[1]
    lo, hi, one, three, here = mixer(where, normed, full, width)

    def wide(a):
        return a.astype(jnp.float32)

    from_left = shift(lo, "x", 4, 1)
    from_right = shift(hi, "x", 4, -1)
    left_hi = shift(one[half:], "x", 4, 1)
    right_lo = shift(three[:half], "x", 4, -1)
    left_lo = shift((wide(one[:half]) + wide(from_left)).astype(jnp.bfloat16), "x", 4, 1)
    right_hi = shift((wide(three[half:]) + wide(from_right)).astype(jnp.bfloat16), "x", 4, -1)
    near = wide(own) + wide(here)
    first = near[:half] + wide(right_lo) + wide(left_lo)
    second = near[half:] + wide(left_hi) + wide(right_hi)
    return jnp.concatenate([first, second], axis=0).astype(jnp.bfloat16)


def solution(mesh):
    fine = Mesh(mesh.devices.reshape(8, 4, 2, 4), ("z", "y", "c", "x"))
    sp = ("z", "y", "c")
    in_specs = (P(sp, "x"),) * 5 + (
        P("x"),
        P("x"),
        P("x", None),
        P(sp, "x"),
        P(),
        P(sp, "x"),
        P(sp, "x"),
        P("x", sp),
    )

    return jax.shard_map(per_device, mesh=fine, in_specs=in_specs, out_specs=P(sp, "x"), check_vma=False)
```

```python
import functools
import math

import jax
import jax.numpy as jnp
from jax import lax
from jax.experimental import pallas as pl
from jax.experimental.pallas import tpu as pltpu
from jax.sharding import Mesh
from jax.sharding import PartitionSpec as P

HEAD = 128
EPS = 1e-06
NEG = -1e30
FLOOR = -1e20
SCALE2 = HEAD**-0.5 * math.log2(math.e)
STAT = 16


VMEM = pl.BlockSpec(memory_space=pltpu.VMEM)
SMEM = pl.BlockSpec(memory_space=pltpu.SMEM)


def shift(a, axis, count, by):
    return lax.ppermute(a, axis, [(i, (i + by) % count) for i in range(count)])


def down_hop(a, hop):
    return lax.ppermute(a, "z", [((b + 1 - hop) % 8, (b - hop) % 8) for b in range(4)])


def dot_nt(a, b):
    return lax.dot_general(a, b, (((1,), (1,)), ((), ())), preferred_element_type=jnp.float32)


def dot_nn(a, b):
    return lax.dot_general(a, b, (((1,), (0,)), ((), ())), preferred_element_type=jnp.float32)


def eye(n):
    return lax.broadcasted_iota(jnp.int32, (n, n), 0) == lax.broadcasted_iota(jnp.int32, (n, n), 1)


def to_row(col):
    n = col.shape[0]
    return jnp.sum(jnp.where(eye(n), col, 0.0), axis=0, keepdims=True)


def to_col(row):
    n = row.shape[1]
    return jnp.sum(jnp.where(eye(n), row, 0.0), axis=1, keepdims=True)


def stat_rows(lse_cols):
    row = jnp.concatenate([to_row(c) for c in lse_cols], axis=1)
    high = row.astype(jnp.bfloat16)
    rest = row - high.astype(jnp.float32)
    mid = rest.astype(jnp.bfloat16)
    low = (rest - mid.astype(jnp.float32)).astype(jnp.bfloat16)
    index = lax.broadcasted_iota(jnp.int32, (STAT, row.shape[1]), 0)
    zero = jnp.zeros_like(row)
    picked = jnp.where(
        index == 0,
        high.astype(jnp.float32),
        jnp.where(index == 1, mid.astype(jnp.float32), jnp.where(index == 2, low.astype(jnp.float32), zero)),
    )
    return picked.astype(jnp.bfloat16)


def read_stats(block, m):
    rows = block.shape[0] - STAT
    half = block.shape[1] // 2
    stats = block[rows:, m * half : (m + 1) * half].astype(jnp.float32)
    return to_col(jnp.sum(stats, axis=0, keepdims=True))


def attention_kernel(steps, carried, where_ref, q_ref, other_q_ref, *rest):
    pieces, rest = rest[: len(steps)], rest[len(steps) :]
    before, (mine_ref, other_ref, s_ref) = rest[:-3], rest[-3:]
    z, y, c = where_ref[0], where_ref[1], where_ref[2]
    r = pl.program_id(0)
    yq = lax.rem(y - r + 4, 4)
    tok = q_ref.shape[1]
    rows = 2 * tok
    lanes = 128
    biases, starts, at = [], [], 0
    for ref, step in zip(pieces, steps):
        source = lax.rem(z + step + 8, 8)
        biases.append(jnp.where(source <= z, 0.0, NEG).astype(jnp.float32))
        starts.append(at)
        at += ref.shape[0]
    out = []
    lse = []
    for m in range(2):
        heads = slice(m * HEAD, (m + 1) * HEAD)
        q = jnp.concatenate([q_ref[0, :, heads], other_q_ref[0, :, heads]], axis=0)
        high = jnp.full((rows, lanes), FLOOR, jnp.float32)
        for n, ref in enumerate(pieces):
            keys = ref.shape[0]
            s = dot_nt(q, ref[:, heads])
            if steps[n] == 0:
                row = lax.broadcasted_iota(jnp.int32, (rows, keys), 0)
                col = lax.broadcasted_iota(jnp.int32, (rows, keys), 1)
                qpos = yq * rows + jnp.where(row < tok, row + c * tok, row - tok + (1 - c) * tok)
                s = jnp.where(y * rows + c * tok + col <= qpos, s, NEG)
            s_ref[:, starts[n] : starts[n] + keys] = s
            top = s[:, :lanes]
            for k in range(lanes, keys, lanes):
                top = jnp.maximum(top, s[:, k : k + lanes])
            high = jnp.maximum(high, top * SCALE2 + biases[n])
        high = jnp.max(high, axis=1, keepdims=True)
        total = jnp.zeros((rows, lanes), jnp.float32)
        acc = jnp.zeros((rows, 2 * HEAD), jnp.float32)
        for n, ref in enumerate(pieces):
            keys = ref.shape[0]
            p = jnp.exp2(s_ref[:, starts[n] : starts[n] + keys] * SCALE2 - (high - biases[n]))
            for k in range(0, keys, lanes):
                total = total + p[:, k : k + lanes]
            acc = acc + dot_nn(p.astype(jnp.bfloat16), ref[:, 2 * HEAD :])
        total = jnp.sum(total, axis=1, keepdims=True)
        if carried:
            stats = jnp.concatenate([read_stats(ref[0], m) for ref in before], axis=0)
            old = jnp.concatenate(
                [ref[0, :tok, m * 2 * HEAD : (m + 1) * 2 * HEAD] for ref in before], axis=0
            )
            now = jnp.where(total > 0.0, high + jnp.log2(jnp.maximum(total, 1e-30)), NEG)
            top = jnp.maximum(stats, now)
            w_old, w_now = jnp.exp2(stats - top), jnp.exp2(now - top)
            both = w_old + w_now
            scale_now = w_now / (jnp.maximum(total, 1e-30) * both)
            out.append((acc * scale_now + old.astype(jnp.float32) * (w_old / both)).astype(jnp.bfloat16))
            lse.append(top + jnp.log2(both))
        else:
            out.append((acc * (1.0 / jnp.maximum(total, 1e-30))).astype(jnp.bfloat16))
            lse.append(jnp.where(total > 0.0, high + jnp.log2(jnp.maximum(total, 1e-30)), NEG))
    for h, ref in enumerate((mine_ref, other_ref)):
        part = slice(h * tok, (h + 1) * tok)
        ref[0, :tok, : 2 * HEAD] = out[0][part]
        ref[0, :tok, 2 * HEAD :] = out[1][part]
        ref[0, tok:, :] = stat_rows([lse[0][part], lse[1][part]])


def attention(where, q, other_q, pieces, steps, before):
    count, tok, _ = q.shape
    rows = 2 * tok
    keys = sum(p.shape[0] for p in pieces)
    width = pieces[0].shape[1]
    block = jax.ShapeDtypeStruct((count, tok + STAT, width), jnp.bfloat16)
    flops = 2 * 2 * count * rows * keys * 3 * HEAD
    spec = pl.BlockSpec((1, tok + STAT, width), lambda r: (r, 0, 0))
    return pl.pallas_call(
        functools.partial(attention_kernel, steps, bool(before)),
        grid=(count,),
        out_shape=(block, block),
        in_specs=[SMEM]
        + [pl.BlockSpec((1, tok, 2 * HEAD), lambda r: (r, 0, 0))] * 2
        + [pl.BlockSpec(p.shape, lambda r: (0, 0)) for p in pieces]
        + [spec] * len(before),
        out_specs=[spec, spec],
        scratch_shapes=[pltpu.VMEM((rows, keys), jnp.float32)],
        compiler_params=pltpu.CompilerParams(vmem_limit_bytes=20 * 1024 * 1024),
        cost_estimate=pl.CostEstimate(
            flops=flops, bytes_accessed=4 * 1024 * 1024, transcendentals=2 * count * rows * keys
        ),
    )(where, q, other_q, *pieces, *before)


def merged(blocks):
    tok = blocks[0].shape[0] - STAT
    stats = [[read_stats(b, m) for m in range(2)] for b in blocks]
    outs, lses = [], []
    for m in range(2):
        top = stats[0][m]
        for s in stats[1:]:
            top = jnp.maximum(top, s[m])
        weights = [jnp.exp2(s[m] - top) for s in stats]
        total = sum(weights[1:], weights[0])
        acc = None
        for w, b in zip(weights, blocks):
            term = w * b[:tok, m * 2 * HEAD : (m + 1) * 2 * HEAD].astype(jnp.float32)
            acc = term if acc is None else acc + term
        outs.append(acc / total)
        lses.append(top + jnp.log2(total))
    return outs, lses


def merge_kernel(a_ref, b_ref, *out_refs):
    for r, ref in enumerate(out_refs):
        tok = ref.shape[0] - STAT
        outs, lses = merged([a_ref[r], b_ref[r]])
        ref[:tok, : 2 * HEAD] = outs[0].astype(jnp.bfloat16)
        ref[:tok, 2 * HEAD :] = outs[1].astype(jnp.bfloat16)
        ref[tok:, :] = stat_rows(lses)


def merge_cores(a, b):
    count, rows, width = a.shape
    return pl.pallas_call(
        merge_kernel,
        out_shape=(jax.ShapeDtypeStruct((rows, width), jnp.bfloat16),) * count,
        in_specs=[VMEM, VMEM],
        out_specs=(VMEM,) * count,
        compiler_params=pltpu.CompilerParams(vmem_limit_bytes=10 * 1024 * 1024),
        cost_estimate=pl.CostEstimate(flops=4_000_000_000, bytes_accessed=3 * a.size * 2, transcendentals=0),
        name="merge_cores",
    )(a, b)


def finish_kernel(lam_ref, gain_ref, *refs):
    blocks, out_ref = [ref[...] for ref in refs[:-1]], refs[-1]
    outs, _ = merged(blocks)
    mixed = outs[0] - lam_ref[0] * outs[1]
    mean = jnp.mean(mixed * mixed, axis=1, keepdims=True)
    out_ref[...] = (mixed * lax.rsqrt(mean + EPS) * gain_ref[...] * 0.8).astype(jnp.bfloat16)


def finish(lam, gain, blocks):
    tok = blocks[0].shape[0] - STAT
    return pl.pallas_call(
        finish_kernel,
        out_shape=jax.ShapeDtypeStruct((tok, 2 * HEAD), jnp.bfloat16),
        in_specs=[SMEM] + [VMEM] * (1 + len(blocks)),
        out_specs=VMEM,
        compiler_params=pltpu.CompilerParams(vmem_limit_bytes=8 * 1024 * 1024),
        cost_estimate=pl.CostEstimate(flops=4_000_000_000, bytes_accessed=2_000_000, transcendentals=0),
        name="finish_heads",
    )(lam, gain.reshape(1, -1), *blocks)


def project_kernel(where_ref, gain_ref, *refs):
    att, (ow_ref, res_ref), extra = refs[:4], refs[4:6], refs[6:12]
    own_ref, normed_ref, sum_ref = refs[12:]
    x = where_ref[3]
    tok, block = res_ref.shape
    width = ow_ref.shape[1]
    half = tok // 2

    def at(s):
        return pl.ds(pl.multiple_of(lax.rem(x - s + 4, 4) * block, block), block)

    sum_ref[:, at(0)] = res_ref[...].astype(jnp.float32)
    for s in range(3):
        sum_ref[:half, at(s + 1)] = extra[2 * s][:, width:].astype(jnp.float32)
        sum_ref[half:, at(s + 1)] = extra[2 * s + 1][:, width:].astype(jnp.float32)
    square = jnp.zeros((tok, 1), jnp.float32)
    for k in range(0, width, block):
        cols = slice(k, k + block)
        acc = sum_ref[:, cols]
        parts = [dot_nn(att[0][...], ow_ref[:, cols])]
        for s in range(3):
            low, high = extra[2 * s], extra[2 * s + 1]
            parts.append(
                dot_nn(att[s + 1][:, :half], low[:, cols]) + dot_nn(att[s + 1][:, half:], high[:, cols])
            )
        total = None
        for part in parts:
            part = part.astype(jnp.bfloat16).astype(jnp.float32)
            total = part if total is None else total + part
        resid = (acc + total).astype(jnp.bfloat16).astype(jnp.float32)
        sum_ref[:, cols] = resid
        square = square + jnp.sum(resid * resid, axis=1, keepdims=True)
    scale = lax.rsqrt(square * (1.0 / width) + EPS)
    own_ref[...] = sum_ref[:, at(0)].astype(jnp.bfloat16)
    normed_ref[...] = (sum_ref[...] * scale * gain_ref[...]).astype(jnp.bfloat16)


def project(where, gain, att, ow, res, extra):
    tok, block = res.shape
    width = ow.shape[1]
    return pl.pallas_call(
        project_kernel,
        out_shape=(
            jax.ShapeDtypeStruct((tok, block), jnp.bfloat16),
            jax.ShapeDtypeStruct((tok, width), jnp.bfloat16),
        ),
        in_specs=[SMEM] + [VMEM] * 13,
        out_specs=(VMEM, VMEM),
        scratch_shapes=[pltpu.VMEM((tok, width), jnp.float32)],
        compiler_params=pltpu.CompilerParams(vmem_limit_bytes=16 * 1024 * 1024),
        cost_estimate=pl.CostEstimate(flops=2_000_000_000, bytes_accessed=8_000_000, transcendentals=0),
        name="project_norm",
    )(where, gain.reshape(1, -1), *att, ow, res, *extra)


def mixer_kernel(where_ref, normed_ref, full_ref, lo_ref, hi_ref, one_ref, three_ref, here_ref, w_ref, d_ref, h_ref, sems):
    count, _, width = w_ref.shape
    _, block, units = d_ref.shape
    lane = width // 2
    half = lo_ref.shape[0]

    def copies(j):
        at = pl.multiple_of(j * lane, lane)
        return [
            pltpu.make_async_copy(
                full_ref.at[:, pl.ds(at + n * units, lane)],
                w_ref.at[j, :, pl.ds(n * lane, lane)],
                sems.at[n, j],
            )
            for n in range(2)
        ]

    def down_copy(n, s):
        row = pl.multiple_of(lax.rem(where_ref[3] + s, 4) * block, block)
        return pltpu.make_async_copy(
            full_ref.at[pl.ds(row, block), pl.ds(2 * units, units)], d_ref.at[n], sems.at[0, count + n]
        )

    @pl.loop(0, count)
    def _(j):
        for c in copies(j):
            c.start()

    ahead = (2, 1, 3, 0)
    for n, s in enumerate(ahead):
        down_copy(n, s).start()

    @pl.loop(0, count)
    def _(j):
        for c in copies(j):
            c.wait()
        both = dot_nn(normed_ref[...], w_ref[j])
        gate, up = both[:, :lane], both[:, lane:]
        cols = pl.ds(pl.multiple_of(j * lane, lane), lane)
        h_ref[:, cols] = (gate / (1.0 + jnp.exp(-gate)) * up).astype(jnp.bfloat16)

    for n, s in enumerate(ahead):
        down_copy(n, s).wait()
    two = dot_nt(h_ref[...], d_ref[0]).astype(jnp.bfloat16)
    lo_ref[...] = two[:half]
    hi_ref[...] = two[half:]
    for n, ref in enumerate((one_ref, three_ref, here_ref)):
        ref[...] = dot_nt(h_ref[...], d_ref[n + 1]).astype(jnp.bfloat16)


def mixer(where, normed, full, block):
    tok, width = normed.shape
    units = full.shape[1] // 3
    lane = 128
    count = units // lane
    whole = jax.ShapeDtypeStruct((tok, block), jnp.bfloat16)
    part = jax.ShapeDtypeStruct((tok // 2, block), jnp.bfloat16)
    return pl.pallas_call(
        mixer_kernel,
        out_shape=(part, part, whole, whole, whole),
        in_specs=[SMEM, VMEM, pl.BlockSpec(memory_space=pl.ANY)],
        out_specs=(VMEM,) * 5,
        scratch_shapes=[
            pltpu.VMEM((count, width, 2 * lane), jnp.bfloat16),
            pltpu.VMEM((4, block, units), jnp.bfloat16),
            pltpu.VMEM((tok, units), jnp.bfloat16),
            pltpu.SemaphoreType.DMA((2, count + 4)),
        ],
        compiler_params=pltpu.CompilerParams(vmem_limit_bytes=48 * 1024 * 1024),
        cost_estimate=pl.CostEstimate(
            flops=2 * tok * width * units * 3, bytes_accessed=18_000_000, transcendentals=tok * units
        ),
        name="mixer",
    )(where, normed, full)


def both_ways(halves, axis, count):
    first, second = halves
    left = [shift(h, axis, count, 1) for h in halves]
    right = [shift(h, axis, count, -1) for h in (second, first)]
    low = shift(left[0], axis, count, 1)
    high = shift(right[0], axis, count, -1)
    return [left[0], left[1], low, high, right[1], right[0]]


def per_device(q1, q2, k1, k2, v, lam, hgain, ow, res, ngain, gw, uw, dw):
    z, y, c, x = (lax.axis_index(n).astype(jnp.int32) for n in ("z", "y", "c", "x"))
    where = jnp.stack([z, y, c, x])

    both = jnp.concatenate([gw, uw, dw.T], axis=1)
    full = lax.all_gather(both, ("z", "y", "c"), axis=0, tiled=True)

    q = jnp.concatenate([q1, q2], axis=1)
    seen = [q]
    for s in range(1, 4):
        seen.append(shift(q, "y", 4, s))
    queries = jnp.stack(seen)
    others = shift(queries, "c", 2, 1)

    kv = jnp.concatenate([k1, k2, v], axis=1)
    tok = kv.shape[0]
    up, down_ring = [kv], [kv]
    for n in range(3):
        up.append(shift(up[-1], "z", 8, 1))
        down_ring.append(down_hop(down_ring[-1], n + 1))
    half_up = shift(up[3][: tok // 2], "z", 8, 1)
    half_down = down_hop(down_ring[3][tok // 2 :], 4)

    half = tok // 2
    extra = both_ways(
        [jnp.concatenate([ow[h : h + half], res[h : h + half]], axis=1) for h in (0, half)], "x", 4
    )

    part = attention(where, queries, others, [kv, up[1], down_ring[1], up[2], down_ring[2]], (0, -1, 1, -2, 2), ())
    mine, other = attention(where, queries, others, [up[3], down_ring[3], half_up, half_down], (-3, 3, 4, 4), part)
    theirs = shift(other, "c", 2, 1)
    blocks = merge_cores(mine, theirs)
    arrived = [blocks[0]] + [shift(blocks[s], "y", 4, -s) for s in range(1, 4)]
    attended = finish(lam, hgain, arrived)
    att = [attended] + [shift(attended, "x", 4, s) for s in range(1, 4)]
    own, normed = project(where, ngain, att, ow, res, extra)

    width = res.shape[1]
    lo, hi, one, three, here = mixer(where, normed, full, width)

    def wide(a):
        return a.astype(jnp.float32)

    from_left = shift(lo, "x", 4, 1)
    from_right = shift(hi, "x", 4, -1)
    left_hi = shift(one[half:], "x", 4, 1)
    right_lo = shift(three[:half], "x", 4, -1)
    left_lo = shift((wide(one[:half]) + wide(from_left)).astype(jnp.bfloat16), "x", 4, 1)
    right_hi = shift((wide(three[half:]) + wide(from_right)).astype(jnp.bfloat16), "x", 4, -1)
    near = wide(own) + wide(here)
    first = near[:half] + wide(right_lo) + wide(left_lo)
    second = near[half:] + wide(left_hi) + wide(right_hi)
    return jnp.concatenate([first, second], axis=0).astype(jnp.bfloat16)


def solution(mesh):
    fine = Mesh(mesh.devices.reshape(8, 4, 2, 4), ("z", "y", "c", "x"))
    sp = ("z", "y", "c")
    in_specs = (P(sp, "x"),) * 5 + (
        P("x"),
        P("x"),
        P("x", None),
        P(sp, "x"),
        P(),
        P(sp, "x"),
        P(sp, "x"),
        P("x", sp),
    )

    return jax.shard_map(per_device, mesh=fine, in_specs=in_specs, out_specs=P(sp, "x"), check_vma=False)
```

```python
import functools
import math

import jax
import jax.numpy as jnp
from jax import lax
from jax.experimental import pallas as pl
from jax.experimental.pallas import tpu as pltpu
from jax.sharding import Mesh
from jax.sharding import PartitionSpec as P

HEAD = 128
EPS = 1e-06
NEG = -1e30
FLOOR = -1e20
SCALE2 = HEAD**-0.5 * math.log2(math.e)
STAT = 16


VMEM = pl.BlockSpec(memory_space=pltpu.VMEM)
SMEM = pl.BlockSpec(memory_space=pltpu.SMEM)


def shift(a, axis, count, by):
    return lax.ppermute(a, axis, [(i, (i + by) % count) for i in range(count)])


def dot_nt(a, b):
    return lax.dot_general(a, b, (((1,), (1,)), ((), ())), preferred_element_type=jnp.float32)


def dot_nn(a, b):
    return lax.dot_general(a, b, (((1,), (0,)), ((), ())), preferred_element_type=jnp.float32)


def eye(n):
    return lax.broadcasted_iota(jnp.int32, (n, n), 0) == lax.broadcasted_iota(jnp.int32, (n, n), 1)


def to_row(col):
    n = col.shape[0]
    return jnp.sum(jnp.where(eye(n), col, 0.0), axis=0, keepdims=True)


def to_col(row):
    n = row.shape[1]
    return jnp.sum(jnp.where(eye(n), row, 0.0), axis=1, keepdims=True)


def stat_rows(lse_cols):
    row = jnp.concatenate([to_row(c) for c in lse_cols], axis=1)
    high = row.astype(jnp.bfloat16)
    rest = row - high.astype(jnp.float32)
    mid = rest.astype(jnp.bfloat16)
    low = (rest - mid.astype(jnp.float32)).astype(jnp.bfloat16)
    index = lax.broadcasted_iota(jnp.int32, (STAT, row.shape[1]), 0)
    zero = jnp.zeros_like(row)
    picked = jnp.where(
        index == 0,
        high.astype(jnp.float32),
        jnp.where(index == 1, mid.astype(jnp.float32), jnp.where(index == 2, low.astype(jnp.float32), zero)),
    )
    return picked.astype(jnp.bfloat16)


def read_stats(block, m):
    rows = block.shape[0] - STAT
    half = block.shape[1] // 2
    stats = block[rows:, m * half : (m + 1) * half].astype(jnp.float32)
    return to_col(jnp.sum(stats, axis=0, keepdims=True))


def attention_kernel(steps, carried, where_ref, q_ref, other_q_ref, *rest):
    pieces, rest = rest[: len(steps)], rest[len(steps) :]
    before, (mine_ref, other_ref, s_ref) = rest[:-3], rest[-3:]
    z, y, c = where_ref[0], where_ref[1], where_ref[2]
    r = pl.program_id(0)
    yq = lax.rem(y - r + 4, 4)
    tok = q_ref.shape[1]
    rows = 2 * tok
    lanes = 128
    biases, starts, at = [], [], 0
    for ref, step in zip(pieces, steps):
        source = lax.rem(z + step + 8, 8)
        biases.append(jnp.where(source <= z, 0.0, NEG).astype(jnp.float32))
        starts.append(at)
        at += ref.shape[0]
    out = []
    lse = []
    for m in range(2):
        heads = slice(m * HEAD, (m + 1) * HEAD)
        q = jnp.concatenate([q_ref[0, :, heads], other_q_ref[0, :, heads]], axis=0)
        high = jnp.full((rows, lanes), FLOOR, jnp.float32)
        for n, ref in enumerate(pieces):
            keys = ref.shape[0]
            s = dot_nt(q, ref[:, heads])
            if steps[n] == 0:
                row = lax.broadcasted_iota(jnp.int32, (rows, keys), 0)
                col = lax.broadcasted_iota(jnp.int32, (rows, keys), 1)
                qpos = yq * rows + jnp.where(row < tok, row + c * tok, row - tok + (1 - c) * tok)
                s = jnp.where(y * rows + c * tok + col <= qpos, s, NEG)
            s_ref[:, starts[n] : starts[n] + keys] = s
            top = s[:, :lanes]
            for k in range(lanes, keys, lanes):
                top = jnp.maximum(top, s[:, k : k + lanes])
            high = jnp.maximum(high, top * SCALE2 + biases[n])
        high = jnp.max(high, axis=1, keepdims=True)
        total = jnp.zeros((rows, lanes), jnp.float32)
        acc = jnp.zeros((rows, 2 * HEAD), jnp.float32)
        for n, ref in enumerate(pieces):
            keys = ref.shape[0]
            p = jnp.exp2(s_ref[:, starts[n] : starts[n] + keys] * SCALE2 - (high - biases[n]))
            for k in range(0, keys, lanes):
                total = total + p[:, k : k + lanes]
            acc = acc + dot_nn(p.astype(jnp.bfloat16), ref[:, 2 * HEAD :])
        total = jnp.sum(total, axis=1, keepdims=True)
        if carried:
            stats = jnp.concatenate([read_stats(ref[0], m) for ref in before], axis=0)
            old = jnp.concatenate(
                [ref[0, :tok, m * 2 * HEAD : (m + 1) * 2 * HEAD] for ref in before], axis=0
            )
            now = jnp.where(total > 0.0, high + jnp.log2(jnp.maximum(total, 1e-30)), NEG)
            top = jnp.maximum(stats, now)
            w_old, w_now = jnp.exp2(stats - top), jnp.exp2(now - top)
            both = w_old + w_now
            scale_now = w_now / (jnp.maximum(total, 1e-30) * both)
            out.append((acc * scale_now + old.astype(jnp.float32) * (w_old / both)).astype(jnp.bfloat16))
            lse.append(top + jnp.log2(both))
        else:
            out.append((acc * (1.0 / jnp.maximum(total, 1e-30))).astype(jnp.bfloat16))
            lse.append(jnp.where(total > 0.0, high + jnp.log2(jnp.maximum(total, 1e-30)), NEG))
    for h, ref in enumerate((mine_ref, other_ref)):
        part = slice(h * tok, (h + 1) * tok)
        ref[0, :tok, : 2 * HEAD] = out[0][part]
        ref[0, :tok, 2 * HEAD :] = out[1][part]
        ref[0, tok:, :] = stat_rows([lse[0][part], lse[1][part]])


def attention(where, q, other_q, pieces, steps, before):
    count, tok, _ = q.shape
    rows = 2 * tok
    keys = sum(p.shape[0] for p in pieces)
    width = pieces[0].shape[1]
    block = jax.ShapeDtypeStruct((count, tok + STAT, width), jnp.bfloat16)
    flops = 2 * 2 * count * rows * keys * 3 * HEAD
    spec = pl.BlockSpec((1, tok + STAT, width), lambda r: (r, 0, 0))
    return pl.pallas_call(
        functools.partial(attention_kernel, steps, bool(before)),
        grid=(count,),
        out_shape=(block, block),
        in_specs=[SMEM]
        + [pl.BlockSpec((1, tok, 2 * HEAD), lambda r: (r, 0, 0))] * 2
        + [pl.BlockSpec(p.shape, lambda r: (0, 0)) for p in pieces]
        + [spec] * len(before),
        out_specs=[spec, spec],
        scratch_shapes=[pltpu.VMEM((rows, keys), jnp.float32)],
        compiler_params=pltpu.CompilerParams(vmem_limit_bytes=20 * 1024 * 1024),
        cost_estimate=pl.CostEstimate(
            flops=flops, bytes_accessed=4 * 1024 * 1024, transcendentals=2 * count * rows * keys
        ),
    )(where, q, other_q, *pieces, *before)


def merged(blocks):
    tok = blocks[0].shape[0] - STAT
    stats = [[read_stats(b, m) for m in range(2)] for b in blocks]
    outs, lses = [], []
    for m in range(2):
        top = stats[0][m]
        for s in stats[1:]:
            top = jnp.maximum(top, s[m])
        weights = [jnp.exp2(s[m] - top) for s in stats]
        total = sum(weights[1:], weights[0])
        acc = None
        for w, b in zip(weights, blocks):
            term = w * b[:tok, m * 2 * HEAD : (m + 1) * 2 * HEAD].astype(jnp.float32)
            acc = term if acc is None else acc + term
        outs.append(acc / total)
        lses.append(top + jnp.log2(total))
    return outs, lses


def merge_kernel(a_ref, b_ref, *out_refs):
    for r, ref in enumerate(out_refs):
        tok = ref.shape[0] - STAT
        outs, lses = merged([a_ref[r], b_ref[r]])
        ref[:tok, : 2 * HEAD] = outs[0].astype(jnp.bfloat16)
        ref[:tok, 2 * HEAD :] = outs[1].astype(jnp.bfloat16)
        ref[tok:, :] = stat_rows(lses)


def merge_cores(a, b):
    count, rows, width = a.shape
    return pl.pallas_call(
        merge_kernel,
        out_shape=(jax.ShapeDtypeStruct((rows, width), jnp.bfloat16),) * count,
        in_specs=[VMEM, VMEM],
        out_specs=(VMEM,) * count,
        compiler_params=pltpu.CompilerParams(vmem_limit_bytes=10 * 1024 * 1024),
        cost_estimate=pl.CostEstimate(flops=4_000_000_000, bytes_accessed=3 * a.size * 2, transcendentals=0),
        name="merge_cores",
    )(a, b)


def finish_kernel(lam_ref, gain_ref, *refs):
    blocks, out_ref = [ref[...] for ref in refs[:-1]], refs[-1]
    outs, _ = merged(blocks)
    mixed = outs[0] - lam_ref[0] * outs[1]
    mean = jnp.mean(mixed * mixed, axis=1, keepdims=True)
    out_ref[...] = (mixed * lax.rsqrt(mean + EPS) * gain_ref[...] * 0.8).astype(jnp.bfloat16)


def finish(lam, gain, blocks):
    tok = blocks[0].shape[0] - STAT
    return pl.pallas_call(
        finish_kernel,
        out_shape=jax.ShapeDtypeStruct((tok, 2 * HEAD), jnp.bfloat16),
        in_specs=[SMEM] + [VMEM] * (1 + len(blocks)),
        out_specs=VMEM,
        compiler_params=pltpu.CompilerParams(vmem_limit_bytes=8 * 1024 * 1024),
        cost_estimate=pl.CostEstimate(flops=4_000_000_000, bytes_accessed=2_000_000, transcendentals=0),
        name="finish_heads",
    )(lam, gain.reshape(1, -1), *blocks)


def project_kernel(where_ref, gain_ref, *refs):
    att, (ow_ref, res_ref), extra = refs[:4], refs[4:6], refs[6:12]
    own_ref, normed_ref, sum_ref = refs[12:]
    x = where_ref[3]
    tok, block = res_ref.shape
    width = ow_ref.shape[1]
    half = tok // 2

    def at(s):
        return pl.ds(pl.multiple_of(lax.rem(x - s + 4, 4) * block, block), block)

    sum_ref[:, at(0)] = res_ref[...].astype(jnp.float32)
    for s in range(3):
        sum_ref[:half, at(s + 1)] = extra[2 * s][:, width:].astype(jnp.float32)
        sum_ref[half:, at(s + 1)] = extra[2 * s + 1][:, width:].astype(jnp.float32)
    square = jnp.zeros((tok, 1), jnp.float32)
    for k in range(0, width, block):
        cols = slice(k, k + block)
        acc = sum_ref[:, cols]
        parts = [dot_nn(att[0][...], ow_ref[:, cols])]
        for s in range(3):
            low, high = extra[2 * s], extra[2 * s + 1]
            parts.append(
                dot_nn(att[s + 1][:, :half], low[:, cols]) + dot_nn(att[s + 1][:, half:], high[:, cols])
            )
        total = None
        for part in parts:
            part = part.astype(jnp.bfloat16).astype(jnp.float32)
            total = part if total is None else total + part
        resid = (acc + total).astype(jnp.bfloat16).astype(jnp.float32)
        sum_ref[:, cols] = resid
        square = square + jnp.sum(resid * resid, axis=1, keepdims=True)
    scale = lax.rsqrt(square * (1.0 / width) + EPS)
    own_ref[...] = sum_ref[:, at(0)].astype(jnp.bfloat16)
    normed_ref[...] = (sum_ref[...] * scale * gain_ref[...]).astype(jnp.bfloat16)


def project(where, gain, att, ow, res, extra):
    tok, block = res.shape
    width = ow.shape[1]
    return pl.pallas_call(
        project_kernel,
        out_shape=(
            jax.ShapeDtypeStruct((tok, block), jnp.bfloat16),
            jax.ShapeDtypeStruct((tok, width), jnp.bfloat16),
        ),
        in_specs=[SMEM] + [VMEM] * 13,
        out_specs=(VMEM, VMEM),
        scratch_shapes=[pltpu.VMEM((tok, width), jnp.float32)],
        compiler_params=pltpu.CompilerParams(vmem_limit_bytes=16 * 1024 * 1024),
        cost_estimate=pl.CostEstimate(flops=2_000_000_000, bytes_accessed=8_000_000, transcendentals=0),
        name="project_norm",
    )(where, gain.reshape(1, -1), *att, ow, res, *extra)


def mixer_kernel(where_ref, normed_ref, full_ref, lo_ref, hi_ref, one_ref, three_ref, here_ref, w_ref, d_ref, h_ref, sems):
    count, _, width = w_ref.shape
    _, block, units = d_ref.shape
    lane = width // 2
    half = lo_ref.shape[0]

    def copies(j):
        at = pl.multiple_of(j * lane, lane)
        return [
            pltpu.make_async_copy(
                full_ref.at[:, pl.ds(at + n * units, lane)],
                w_ref.at[j, :, pl.ds(n * lane, lane)],
                sems.at[n, j],
            )
            for n in range(2)
        ]

    def down_copy(n, s):
        row = pl.multiple_of(lax.rem(where_ref[3] + s, 4) * block, block)
        return pltpu.make_async_copy(
            full_ref.at[pl.ds(row, block), pl.ds(2 * units, units)], d_ref.at[n], sems.at[0, count + n]
        )

    @pl.loop(0, count)
    def _(j):
        for c in copies(j):
            c.start()

    ahead = (2, 1, 3, 0)
    for n, s in enumerate(ahead):
        down_copy(n, s).start()

    @pl.loop(0, count)
    def _(j):
        for c in copies(j):
            c.wait()
        both = dot_nn(normed_ref[...], w_ref[j])
        gate, up = both[:, :lane], both[:, lane:]
        cols = pl.ds(pl.multiple_of(j * lane, lane), lane)
        h_ref[:, cols] = (gate / (1.0 + jnp.exp(-gate)) * up).astype(jnp.bfloat16)

    down_copy(0, ahead[0]).wait()
    two = dot_nt(h_ref[...], d_ref[0]).astype(jnp.bfloat16)
    lo_ref[...] = two[:half]
    hi_ref[...] = two[half:]
    for n, ref in enumerate((one_ref, three_ref, here_ref)):
        down_copy(n + 1, ahead[n + 1]).wait()
        ref[...] = dot_nt(h_ref[...], d_ref[n + 1]).astype(jnp.bfloat16)


def mixer(where, normed, full, block):
    tok, width = normed.shape
    units = full.shape[1] // 3
    lane = 128
    count = units // lane
    whole = jax.ShapeDtypeStruct((tok, block), jnp.bfloat16)
    part = jax.ShapeDtypeStruct((tok // 2, block), jnp.bfloat16)
    return pl.pallas_call(
        mixer_kernel,
        out_shape=(part, part, whole, whole, whole),
        in_specs=[SMEM, VMEM, pl.BlockSpec(memory_space=pl.ANY)],
        out_specs=(VMEM,) * 5,
        scratch_shapes=[
            pltpu.VMEM((count, width, 2 * lane), jnp.bfloat16),
            pltpu.VMEM((4, block, units), jnp.bfloat16),
            pltpu.VMEM((tok, units), jnp.bfloat16),
            pltpu.SemaphoreType.DMA((2, count + 4)),
        ],
        compiler_params=pltpu.CompilerParams(vmem_limit_bytes=48 * 1024 * 1024),
        cost_estimate=pl.CostEstimate(
            flops=2 * tok * width * units * 3, bytes_accessed=18_000_000, transcendentals=tok * units
        ),
        name="mixer",
    )(where, normed, full)


def both_ways(halves, axis, count):
    first, second = halves
    left = [shift(h, axis, count, 1) for h in halves]
    right = [shift(h, axis, count, -1) for h in (second, first)]
    low = shift(left[0], axis, count, 1)
    high = shift(right[0], axis, count, -1)
    return [left[0], left[1], low, high, right[1], right[0]]


def per_device(q1, q2, k1, k2, v, lam, hgain, ow, res, ngain, gw, uw, dw):
    z, y, c, x = (lax.axis_index(n).astype(jnp.int32) for n in ("z", "y", "c", "x"))
    where = jnp.stack([z, y, c, x])

    both = jnp.concatenate([gw, uw, dw.T], axis=1)
    full = lax.all_gather(both, ("z", "y", "c"), axis=0, tiled=True)

    q = jnp.concatenate([q1, q2], axis=1)
    seen = [q]
    for s in range(1, 4):
        seen.append(shift(q, "y", 4, s))
    queries = jnp.stack(seen)
    others = shift(queries, "c", 2, 1)

    kv = jnp.concatenate([k1, k2, v], axis=1)
    tok = kv.shape[0]
    up, down_ring = [kv], [kv]
    for _ in range(3):
        up.append(shift(up[-1], "z", 8, 1))
        down_ring.append(shift(down_ring[-1], "z", 8, -1))
    half_up = shift(up[3][: tok // 2], "z", 8, 1)
    half_down = shift(down_ring[3][tok // 2 :], "z", 8, -1)

    half = tok // 2
    extra = both_ways(
        [jnp.concatenate([ow[h : h + half], res[h : h + half]], axis=1) for h in (0, half)], "x", 4
    )

    part = attention(where, queries, others, [kv, up[1], down_ring[1], up[2], down_ring[2]], (0, -1, 1, -2, 2), ())
    mine, other = attention(where, queries, others, [up[3], down_ring[3], half_up, half_down], (-3, 3, 4, 4), part)
    theirs = shift(other, "c", 2, 1)
    blocks = merge_cores(mine, theirs)
    arrived = [blocks[0]] + [shift(blocks[s], "y", 4, -s) for s in range(1, 4)]
    attended = finish(lam, hgain, arrived)
    att = [attended] + [shift(attended, "x", 4, s) for s in range(1, 4)]
    own, normed = project(where, ngain, att, ow, res, extra)

    width = res.shape[1]
    lo, hi, one, three, here = mixer(where, normed, full, width)

    def wide(a):
        return a.astype(jnp.float32)

    from_left = shift(lo, "x", 4, 1)
    from_right = shift(hi, "x", 4, -1)
    left_hi = shift(one[half:], "x", 4, 1)
    right_lo = shift(three[:half], "x", 4, -1)
    left_lo = shift((wide(one[:half]) + wide(from_left)).astype(jnp.bfloat16), "x", 4, 1)
    right_hi = shift((wide(three[half:]) + wide(from_right)).astype(jnp.bfloat16), "x", 4, -1)
    near = wide(own) + wide(here)
    first = near[:half] + wide(right_lo) + wide(left_lo)
    second = near[half:] + wide(left_hi) + wide(right_hi)
    return jnp.concatenate([first, second], axis=0).astype(jnp.bfloat16)


def solution(mesh):
    fine = Mesh(mesh.devices.reshape(8, 4, 2, 4), ("z", "y", "c", "x"))
    sp = ("z", "y", "c")
    in_specs = (P(sp, "x"),) * 5 + (
        P("x"),
        P("x"),
        P("x", None),
        P(sp, "x"),
        P(),
        P(sp, "x"),
        P(sp, "x"),
        P("x", sp),
    )

    return jax.shard_map(per_device, mesh=fine, in_specs=in_specs, out_specs=P(sp, "x"), check_vma=False)
```

```python
import functools
import math

import jax
import jax.numpy as jnp
from jax import lax
from jax.experimental import pallas as pl
from jax.experimental.pallas import tpu as pltpu
from jax.sharding import Mesh
from jax.sharding import PartitionSpec as P

HEAD = 128
EPS = 1e-06
NEG = -1e30
FLOOR = -1e20
SCALE2 = HEAD**-0.5 * math.log2(math.e)
STAT = 16


VMEM = pl.BlockSpec(memory_space=pltpu.VMEM)
SMEM = pl.BlockSpec(memory_space=pltpu.SMEM)


def shift(a, axis, count, by):
    return lax.ppermute(a, axis, [(i, (i + by) % count) for i in range(count)])


def dot_nt(a, b):
    return lax.dot_general(a, b, (((1,), (1,)), ((), ())), preferred_element_type=jnp.float32)


def dot_nn(a, b):
    return lax.dot_general(a, b, (((1,), (0,)), ((), ())), preferred_element_type=jnp.float32)


def eye(n):
    return lax.broadcasted_iota(jnp.int32, (n, n), 0) == lax.broadcasted_iota(jnp.int32, (n, n), 1)


def to_row(col):
    n = col.shape[0]
    return jnp.sum(jnp.where(eye(n), col, 0.0), axis=0, keepdims=True)


def to_col(row):
    n = row.shape[1]
    return jnp.sum(jnp.where(eye(n), row, 0.0), axis=1, keepdims=True)


def stat_rows(lse_cols):
    row = jnp.concatenate([to_row(c) for c in lse_cols], axis=1)
    high = row.astype(jnp.bfloat16)
    rest = row - high.astype(jnp.float32)
    mid = rest.astype(jnp.bfloat16)
    low = (rest - mid.astype(jnp.float32)).astype(jnp.bfloat16)
    index = lax.broadcasted_iota(jnp.int32, (STAT, row.shape[1]), 0)
    zero = jnp.zeros_like(row)
    picked = jnp.where(
        index == 0,
        high.astype(jnp.float32),
        jnp.where(index == 1, mid.astype(jnp.float32), jnp.where(index == 2, low.astype(jnp.float32), zero)),
    )
    return picked.astype(jnp.bfloat16)


def read_stats(block, m):
    rows = block.shape[0] - STAT
    half = block.shape[1] // 2
    stats = block[rows:, m * half : (m + 1) * half].astype(jnp.float32)
    return to_col(jnp.sum(stats, axis=0, keepdims=True))


def attention_kernel(steps, carried, where_ref, q_ref, other_q_ref, *rest):
    pieces, rest = rest[: len(steps)], rest[len(steps) :]
    before, (mine_ref, other_ref, s_ref) = rest[:-3], rest[-3:]
    z, y, c = where_ref[0], where_ref[1], where_ref[2]
    r = pl.program_id(0)
    yq = lax.rem(y - r + 4, 4)
    tok = q_ref.shape[1]
    rows = 2 * tok
    lanes = 128
    biases, starts, at = [], [], 0
    for ref, step in zip(pieces, steps):
        source = lax.rem(z + step + 8, 8)
        biases.append(jnp.where(source <= z, 0.0, NEG).astype(jnp.float32))
        starts.append(at)
        at += ref.shape[0]
    out = []
    lse = []
    for m in range(2):
        heads = slice(m * HEAD, (m + 1) * HEAD)
        q = jnp.concatenate([q_ref[0, :, heads], other_q_ref[0, :, heads]], axis=0)
        high = jnp.full((rows, lanes), FLOOR, jnp.float32)
        for n, ref in enumerate(pieces):
            keys = ref.shape[0]
            s = dot_nt(q, ref[:, heads])
            if steps[n] == 0:
                row = lax.broadcasted_iota(jnp.int32, (rows, keys), 0)
                col = lax.broadcasted_iota(jnp.int32, (rows, keys), 1)
                qpos = yq * rows + jnp.where(row < tok, row + c * tok, row - tok + (1 - c) * tok)
                s = jnp.where(y * rows + c * tok + col <= qpos, s, NEG)
            s_ref[:, starts[n] : starts[n] + keys] = s
            top = s[:, :lanes]
            for k in range(lanes, keys, lanes):
                top = jnp.maximum(top, s[:, k : k + lanes])
            high = jnp.maximum(high, top * SCALE2 + biases[n])
        high = jnp.max(high, axis=1, keepdims=True)
        total = jnp.zeros((rows, lanes), jnp.float32)
        acc = jnp.zeros((rows, 2 * HEAD), jnp.float32)
        for n, ref in enumerate(pieces):
            keys = ref.shape[0]
            p = jnp.exp2(s_ref[:, starts[n] : starts[n] + keys] * SCALE2 - (high - biases[n]))
            for k in range(0, keys, lanes):
                total = total + p[:, k : k + lanes]
            acc = acc + dot_nn(p.astype(jnp.bfloat16), ref[:, 2 * HEAD :])
        total = jnp.sum(total, axis=1, keepdims=True)
        if carried:
            stats = jnp.concatenate([read_stats(ref[0], m) for ref in before], axis=0)
            old = jnp.concatenate(
                [ref[0, :tok, m * 2 * HEAD : (m + 1) * 2 * HEAD] for ref in before], axis=0
            )
            now = jnp.where(total > 0.0, high + jnp.log2(jnp.maximum(total, 1e-30)), NEG)
            top = jnp.maximum(stats, now)
            w_old, w_now = jnp.exp2(stats - top), jnp.exp2(now - top)
            both = w_old + w_now
            scale_now = w_now / (jnp.maximum(total, 1e-30) * both)
            out.append((acc * scale_now + old.astype(jnp.float32) * (w_old / both)).astype(jnp.bfloat16))
            lse.append(top + jnp.log2(both))
        else:
            out.append((acc * (1.0 / jnp.maximum(total, 1e-30))).astype(jnp.bfloat16))
            lse.append(jnp.where(total > 0.0, high + jnp.log2(jnp.maximum(total, 1e-30)), NEG))
    for h, ref in enumerate((mine_ref, other_ref)):
        part = slice(h * tok, (h + 1) * tok)
        ref[0, :tok, : 2 * HEAD] = out[0][part]
        ref[0, :tok, 2 * HEAD :] = out[1][part]
        ref[0, tok:, :] = stat_rows([lse[0][part], lse[1][part]])


def attention(where, q, other_q, pieces, steps, before):
    count, tok, _ = q.shape
    rows = 2 * tok
    keys = sum(p.shape[0] for p in pieces)
    width = pieces[0].shape[1]
    block = jax.ShapeDtypeStruct((count, tok + STAT, width), jnp.bfloat16)
    flops = 2 * 2 * count * rows * keys * 3 * HEAD
    spec = pl.BlockSpec((1, tok + STAT, width), lambda r: (r, 0, 0))
    return pl.pallas_call(
        functools.partial(attention_kernel, steps, bool(before)),
        grid=(count,),
        out_shape=(block, block),
        in_specs=[SMEM]
        + [pl.BlockSpec((1, tok, 2 * HEAD), lambda r: (r, 0, 0))] * 2
        + [pl.BlockSpec(p.shape, lambda r: (0, 0)) for p in pieces]
        + [spec] * len(before),
        out_specs=[spec, spec],
        scratch_shapes=[pltpu.VMEM((rows, keys), jnp.float32)],
        compiler_params=pltpu.CompilerParams(vmem_limit_bytes=20 * 1024 * 1024),
        cost_estimate=pl.CostEstimate(
            flops=flops, bytes_accessed=4 * 1024 * 1024, transcendentals=2 * count * rows * keys
        ),
    )(where, q, other_q, *pieces, *before)


def merged(blocks):
    tok = blocks[0].shape[0] - STAT
    stats = [[read_stats(b, m) for m in range(2)] for b in blocks]
    outs, lses = [], []
    for m in range(2):
        top = stats[0][m]
        for s in stats[1:]:
            top = jnp.maximum(top, s[m])
        weights = [jnp.exp2(s[m] - top) for s in stats]
        total = sum(weights[1:], weights[0])
        acc = None
        for w, b in zip(weights, blocks):
            term = w * b[:tok, m * 2 * HEAD : (m + 1) * 2 * HEAD].astype(jnp.float32)
            acc = term if acc is None else acc + term
        outs.append(acc / total)
        lses.append(top + jnp.log2(total))
    return outs, lses


def merge_kernel(a_ref, b_ref, *out_refs):
    for r, ref in enumerate(out_refs):
        tok = ref.shape[0] - STAT
        outs, lses = merged([a_ref[r], b_ref[r]])
        ref[:tok, : 2 * HEAD] = outs[0].astype(jnp.bfloat16)
        ref[:tok, 2 * HEAD :] = outs[1].astype(jnp.bfloat16)
        ref[tok:, :] = stat_rows(lses)


def merge_cores(a, b):
    count, rows, width = a.shape
    return pl.pallas_call(
        merge_kernel,
        out_shape=(jax.ShapeDtypeStruct((rows, width), jnp.bfloat16),) * count,
        in_specs=[VMEM, VMEM],
        out_specs=(VMEM,) * count,
        compiler_params=pltpu.CompilerParams(vmem_limit_bytes=10 * 1024 * 1024),
        cost_estimate=pl.CostEstimate(flops=4_000_000_000, bytes_accessed=3 * a.size * 2, transcendentals=0),
        name="merge_cores",
    )(a, b)


def finish_kernel(lam_ref, gain_ref, *refs):
    blocks, out_ref = [ref[...] for ref in refs[:-1]], refs[-1]
    outs, _ = merged(blocks)
    mixed = outs[0] - lam_ref[0] * outs[1]
    mean = jnp.mean(mixed * mixed, axis=1, keepdims=True)
    out_ref[...] = (mixed * lax.rsqrt(mean + EPS) * gain_ref[...] * 0.8).astype(jnp.bfloat16)


def finish(lam, gain, blocks):
    tok = blocks[0].shape[0] - STAT
    return pl.pallas_call(
        finish_kernel,
        out_shape=jax.ShapeDtypeStruct((tok, 2 * HEAD), jnp.bfloat16),
        in_specs=[SMEM] + [VMEM] * (1 + len(blocks)),
        out_specs=VMEM,
        compiler_params=pltpu.CompilerParams(vmem_limit_bytes=8 * 1024 * 1024),
        cost_estimate=pl.CostEstimate(flops=4_000_000_000, bytes_accessed=2_000_000, transcendentals=0),
        name="finish_heads",
    )(lam, gain.reshape(1, -1), *blocks)


def project_kernel(where_ref, gain_ref, *refs):
    att, (ow_ref, res_ref), extra = refs[:4], refs[4:6], refs[6:12]
    own_ref, normed_ref, sum_ref = refs[12:]
    x = where_ref[3]
    tok, block = res_ref.shape
    width = ow_ref.shape[1]
    half = tok // 2

    def at(s):
        return pl.ds(pl.multiple_of(lax.rem(x - s + 4, 4) * block, block), block)

    sum_ref[:, at(0)] = res_ref[...].astype(jnp.float32)
    for s in range(3):
        sum_ref[:half, at(s + 1)] = extra[2 * s][:, width:].astype(jnp.float32)
        sum_ref[half:, at(s + 1)] = extra[2 * s + 1][:, width:].astype(jnp.float32)
    square = jnp.zeros((tok, 1), jnp.float32)
    for k in range(0, width, block):
        cols = slice(k, k + block)
        acc = sum_ref[:, cols]
        parts = [dot_nn(att[0][...], ow_ref[:, cols])]
        for s in range(3):
            low, high = extra[2 * s], extra[2 * s + 1]
            parts.append(
                dot_nn(att[s + 1][:, :half], low[:, cols]) + dot_nn(att[s + 1][:, half:], high[:, cols])
            )
        total = None
        for part in parts:
            part = part.astype(jnp.bfloat16).astype(jnp.float32)
            total = part if total is None else total + part
        resid = (acc + total).astype(jnp.bfloat16).astype(jnp.float32)
        sum_ref[:, cols] = resid
        square = square + jnp.sum(resid * resid, axis=1, keepdims=True)
    scale = lax.rsqrt(square * (1.0 / width) + EPS)
    own_ref[...] = sum_ref[:, at(0)].astype(jnp.bfloat16)
    normed_ref[...] = (sum_ref[...] * scale * gain_ref[...]).astype(jnp.bfloat16)


def project(where, gain, att, ow, res, extra):
    tok, block = res.shape
    width = ow.shape[1]
    return pl.pallas_call(
        project_kernel,
        out_shape=(
            jax.ShapeDtypeStruct((tok, block), jnp.bfloat16),
            jax.ShapeDtypeStruct((tok, width), jnp.bfloat16),
        ),
        in_specs=[SMEM] + [VMEM] * 13,
        out_specs=(VMEM, VMEM),
        scratch_shapes=[pltpu.VMEM((tok, width), jnp.float32)],
        compiler_params=pltpu.CompilerParams(vmem_limit_bytes=16 * 1024 * 1024),
        cost_estimate=pl.CostEstimate(flops=2_000_000_000, bytes_accessed=8_000_000, transcendentals=0),
        name="project_norm",
    )(where, gain.reshape(1, -1), *att, ow, res, *extra)


def mixer_kernel(where_ref, normed_ref, full_ref, lo_ref, hi_ref, one_ref, three_ref, here_ref, w_ref, d_ref, h_ref, sems):
    count, _, width = w_ref.shape
    _, block, units = d_ref.shape
    lane = width // 2
    half = lo_ref.shape[0]

    def copies(j):
        at = pl.multiple_of(j * width, width)
        return [pltpu.make_async_copy(full_ref.at[:, pl.ds(at, width)], w_ref.at[j], sems.at[0, j])]

    def down_copy(n, s):
        row = pl.multiple_of(lax.rem(where_ref[3] + s, 4) * block, block)
        return pltpu.make_async_copy(
            full_ref.at[pl.ds(row, block), pl.ds(2 * units, units)], d_ref.at[n], sems.at[0, count + n]
        )

    @pl.loop(0, count)
    def _(j):
        for c in copies(j):
            c.start()

    ahead = (2, 1, 3, 0)
    for n, s in enumerate(ahead):
        down_copy(n, s).start()

    @pl.loop(0, count)
    def _(j):
        for c in copies(j):
            c.wait()
        both = dot_nn(normed_ref[...], w_ref[j])
        gate, up = both[:, :lane], both[:, lane:]
        cols = pl.ds(pl.multiple_of(j * lane, lane), lane)
        h_ref[:, cols] = (gate / (1.0 + jnp.exp(-gate)) * up).astype(jnp.bfloat16)

    down_copy(0, ahead[0]).wait()
    two = dot_nt(h_ref[...], d_ref[0]).astype(jnp.bfloat16)
    lo_ref[...] = two[:half]
    hi_ref[...] = two[half:]
    for n, ref in enumerate((one_ref, three_ref, here_ref)):
        down_copy(n + 1, ahead[n + 1]).wait()
        ref[...] = dot_nt(h_ref[...], d_ref[n + 1]).astype(jnp.bfloat16)


def mixer(where, normed, full, block):
    tok, width = normed.shape
    units = full.shape[1] // 3
    lane = 128
    count = units // lane
    whole = jax.ShapeDtypeStruct((tok, block), jnp.bfloat16)
    part = jax.ShapeDtypeStruct((tok // 2, block), jnp.bfloat16)
    return pl.pallas_call(
        mixer_kernel,
        out_shape=(part, part, whole, whole, whole),
        in_specs=[SMEM, VMEM, pl.BlockSpec(memory_space=pl.ANY)],
        out_specs=(VMEM,) * 5,
        scratch_shapes=[
            pltpu.VMEM((count, width, 2 * lane), jnp.bfloat16),
            pltpu.VMEM((4, block, units), jnp.bfloat16),
            pltpu.VMEM((tok, units), jnp.bfloat16),
            pltpu.SemaphoreType.DMA((2, count + 4)),
        ],
        compiler_params=pltpu.CompilerParams(vmem_limit_bytes=48 * 1024 * 1024),
        cost_estimate=pl.CostEstimate(
            flops=2 * tok * width * units * 3, bytes_accessed=18_000_000, transcendentals=tok * units
        ),
        name="mixer",
    )(where, normed, full)


def both_ways(halves, axis, count):
    first, second = halves
    left = [shift(h, axis, count, 1) for h in halves]
    right = [shift(h, axis, count, -1) for h in (second, first)]
    low = shift(left[0], axis, count, 1)
    high = shift(right[0], axis, count, -1)
    return [left[0], left[1], low, high, right[1], right[0]]


def per_device(q1, q2, k1, k2, v, lam, hgain, ow, res, ngain, gw, uw, dw):
    z, y, c, x = (lax.axis_index(n).astype(jnp.int32) for n in ("z", "y", "c", "x"))
    where = jnp.stack([z, y, c, x])

    lane = 128
    blocks = [w.reshape(w.shape[0], -1, lane) for w in (gw, uw)]
    turns = jnp.stack(blocks, axis=2).reshape(gw.shape[0], -1)
    both = jnp.concatenate([turns, dw.T], axis=1)
    full = lax.all_gather(both, ("z", "y", "c"), axis=0, tiled=True)

    q = jnp.concatenate([q1, q2], axis=1)
    seen = [q]
    for s in range(1, 4):
        seen.append(shift(q, "y", 4, s))
    queries = jnp.stack(seen)
    others = shift(queries, "c", 2, 1)

    kv = jnp.concatenate([k1, k2, v], axis=1)
    tok = kv.shape[0]
    up, down_ring = [kv], [kv]
    for _ in range(3):
        up.append(shift(up[-1], "z", 8, 1))
        down_ring.append(shift(down_ring[-1], "z", 8, -1))
    half_up = shift(up[3][: tok // 2], "z", 8, 1)
    half_down = shift(down_ring[3][tok // 2 :], "z", 8, -1)

    half = tok // 2
    extra = both_ways(
        [jnp.concatenate([ow[h : h + half], res[h : h + half]], axis=1) for h in (0, half)], "x", 4
    )

    part = attention(where, queries, others, [kv, up[1], down_ring[1], up[2], down_ring[2]], (0, -1, 1, -2, 2), ())
    mine, other = attention(where, queries, others, [up[3], down_ring[3], half_up, half_down], (-3, 3, 4, 4), part)
    theirs = shift(other, "c", 2, 1)
    blocks = merge_cores(mine, theirs)
    arrived = [blocks[0]] + [shift(blocks[s], "y", 4, -s) for s in range(1, 4)]
    attended = finish(lam, hgain, arrived)
    att = [attended] + [shift(attended, "x", 4, s) for s in range(1, 4)]
    own, normed = project(where, ngain, att, ow, res, extra)

    width = res.shape[1]
    lo, hi, one, three, here = mixer(where, normed, full, width)

    def wide(a):
        return a.astype(jnp.float32)

    from_left = shift(lo, "x", 4, 1)
    from_right = shift(hi, "x", 4, -1)
    left_hi = shift(one[half:], "x", 4, 1)
    right_lo = shift(three[:half], "x", 4, -1)
    left_lo = shift((wide(one[:half]) + wide(from_left)).astype(jnp.bfloat16), "x", 4, 1)
    right_hi = shift((wide(three[half:]) + wide(from_right)).astype(jnp.bfloat16), "x", 4, -1)
    near = wide(own) + wide(here)
    first = near[:half] + wide(right_lo) + wide(left_lo)
    second = near[half:] + wide(left_hi) + wide(right_hi)
    return jnp.concatenate([first, second], axis=0).astype(jnp.bfloat16)


def solution(mesh):
    fine = Mesh(mesh.devices.reshape(8, 4, 2, 4), ("z", "y", "c", "x"))
    sp = ("z", "y", "c")
    in_specs = (P(sp, "x"),) * 5 + (
        P("x"),
        P("x"),
        P("x", None),
        P(sp, "x"),
        P(),
        P(sp, "x"),
        P(sp, "x"),
        P("x", sp),
    )

    return jax.shard_map(per_device, mesh=fine, in_specs=in_specs, out_specs=P(sp, "x"), check_vma=False)
```
